128 devices in a mesh: sp: 16 (over z, x), tp: 8 (over y, core).
Axes of the slice: x: 4, y: 4, z: 4, core: 2. Of those that a mesh axis runs over, the one named last changes fastest.
Arguments:
- queries: bfloat16 [8192, 2048], P('sp', 'tp'), may hold values from -6 to 6
- keys: bfloat16 [8192, 1024], P('sp', 'tp'), may hold values from -6 to 6
- values: bfloat16 [8192, 1024], P('sp', 'tp'), may hold values from -6 to 6
- documents: int32 [8192], P('sp'), may hold values from 0 to 3, never falling along the last dimension, each value on 1 to 4096 neighbouring positions
- query_gain: float32 [128], replicated, may hold values from 1.8 to 6
- key_gain: float32 [128], replicated, may hold values from 1.8 to 6
- residual: bfloat16 [8192, 4096], P('sp', 'tp'), may hold values from -6 to 6
- out_weight: bfloat16 [2048, 4096], P('tp'), may hold values from -0.125 to 0.125
- norm_gain: float32 [4096], replicated, may hold values from 0.1 to 1.9
- up_weight: bfloat16 [4096, 16384], P('sp', 'tp'), may hold values from -0.09375 to 0.09375
- down_weight: bfloat16 [16384, 4096], P('tp', 'sp'), may hold values from -0.046875 to 0.046875
Outputs:
- mixed: bfloat16 [8192, 4096], P('sp', 'tp')
The draws below stay inside these ranges and needn't reach their ends.
Inputs may be any that keep to these rules, and one draw needn't show every extreme that they name: `documents`: document numbers never fall along the sequence; a document has at most 4096 positions.
All inputs are finite; a program needn't handle non-finite values.
Results may differ from the reference program's by a relative error of at most 0.017.
The reference program's roundings to bfloat16 on the way count: a program that leaves them out, or rounds other values in their place, can miss the bound.
Values may be sent and summed in bfloat16 or wider, within the bound.
A program may use at most 192 MiB of HBM per device.

```python
import math
import jax
import jax.numpy as jnp
import numpy as np
from jax import lax

D = 4096
FF = 16384
HQ = 16
KV = 8
HD = 128
GRID_W = 64
TOK_DEV = 512
TOKENS = 8192
DOCS = 4
DOC_MOST = 4096
N_SP = 16
N_TP = 8


def drawn_keys(key):
    base = jnp.clip(jax.random.normal(jax.random.fold_in(key, 11), (TOKENS, KV * HD), jnp.float32), -6.0, 6.0)
    return base


def draw_keys(key, part):
    return drawn_keys(key).astype(jnp.bfloat16)


def draw_queries(key, part):
    base = jnp.clip(jax.random.normal(jax.random.fold_in(key, 12), (TOKENS, HQ * HD), jnp.float32), -6.0, 6.0)
    return base.astype(jnp.bfloat16)


def gain_values(key, offset):
    return jax.random.uniform(jax.random.fold_in(key, offset), (HD,), jnp.float32, 1.8, 3.0)


def draw_query_gain(key, part):
    return gain_values(key, 21)


def draw_key_gain(key, part):
    return gain_values(key, 22)


def steps_of(rng, dims, cuts, smallest, top_value):
    def one(axis_at, blocks):
        steps = jax.random.uniform(jax.random.fold_in(jax.random.fold_in(rng, 6), axis_at), (blocks,), jnp.float32, smallest / len(cuts), top_value / len(cuts))
        return jnp.repeat(jnp.exp(steps), dims[axis_at] // blocks).reshape((-1,) + (1,) * (len(dims) - axis_at - 1))

    level = one(*cuts[0])
    for cut in cuts[1:]:
        level = level * one(*cut)
    return level


def split_up(count, total, bound, skew):
    loads = [(1 << 20) // math.isqrt(rank ** skew) + 1 for rank in range(2, count + 1)]
    rest, counts = total - bound - (count - 1), [1] * (count - 1)
    while rest > 0:
        movable = [i for i in range(count - 1) if counts[i] < bound]
        pool, remaining = sum([loads[i] for i in movable]), rest
        for i in movable:
            extra = min(bound - counts[i], max(1, remaining * loads[i] // pool), rest)
            counts[i] = counts[i] + extra
            rest = rest - extra
    return np.array([bound] + counts)


def ragged_sizes(own_key, amount, total, bound, slope):
    if amount == 2:
        one = jax.random.randint(own_key, (), max(1, total - bound), min(bound, total - 1) + 1)
        return jnp.stack([one, total - one])
    sizes = jnp.asarray(split_up(amount, total, bound, slope), jnp.int32)
    couples = (amount - 1) // 2
    giver, receiver = sizes[1:1 + 2 * couples:2], sizes[2:2 + 2 * couples:2]
    margin = jnp.minimum(giver - 1, bound - receiver)
    passed = jax.random.randint(jax.random.fold_in(own_key, 1), (couples,), 0, 1 << 20) % (margin + 1)
    sizes = sizes.at[1:1 + 2 * couples:2].set(giver - passed).at[2:2 + 2 * couples:2].set(receiver + passed)
    return sizes[jax.random.permutation(jax.random.fold_in(own_key, 2), amount)]


def scatter_about(own_key, shape, spread, bound, split=(), kind=jnp.bfloat16):
    level = steps_of(own_key, shape, split, -0.22, 0.18) if split else 1.0
    values = jax.random.normal(own_key, shape, jnp.float32) * spread * level
    return jnp.minimum(jnp.maximum(values, -bound), bound).astype(kind)


def setup_inputs(seed: int = 0) -> dict:
    seeds = jax.random.split(jax.random.key(seed), 12)
    return {
        "queries": draw_queries(jax.random.fold_in(seeds[11], 71), 0),
        "keys": draw_keys(jax.random.fold_in(seeds[11], 71), 0),
        "values": scatter_about(seeds[2], (TOKENS, KV * HD), 1.0, 6.0, ((0, 16), (1, 8))),
        "documents": jnp.searchsorted(jnp.cumsum(ragged_sizes(seeds[3], DOCS, TOKENS, DOC_MOST, 0)), jnp.arange(TOKENS), side="right").astype(jnp.int32),
        "query_gain": draw_query_gain(jax.random.fold_in(seeds[11], 71), 0),
        "key_gain": draw_key_gain(jax.random.fold_in(seeds[11], 71), 0),
        "residual": scatter_about(seeds[6], (TOKENS, D), 1.0, 6.0, ((0, 16), (1, 8))),
        "out_weight": scatter_about(seeds[7], (HQ * HD, D), (HQ * HD) ** -0.5, 0.125, ((0, 8),)),
        "norm_gain": jnp.clip(1.0 + 0.18 * jax.random.normal(seeds[8], (D,), jnp.float32), 0.1, 1.9),
        "up_weight": scatter_about(seeds[9], (D, FF), D ** -0.5, 0.09375, ((0, 16), (1, 8))),
        "down_weight": scatter_about(seeds[10], (FF, D), FF ** -0.5, 0.046875, ((0, 8), (1, 16))),
    }


norm_eps = 1e-06
rope_base = 10000.0
masked_score = -1e+30

def head_norm(heads_in, gain):
    values32 = heads_in.astype(jnp.float32)
    scaled = values32 * lax.rsqrt(lax.optimization_barrier(jnp.mean(values32 * values32, axis=-1, keepdims=True)) + norm_eps)
    return scaled * gain.astype(jnp.float32)

def rotate_half(heads_in, position):
    quarter = heads_in.shape[-1] // 2
    inverse_freq = rope_base ** (-jnp.arange(quarter, dtype=jnp.float32) / quarter)
    angles = position[:, None] * inverse_freq[None, :]
    cosine_part = jnp.cos(angles)[:, None, :]
    sine_part = jnp.sin(angles)[:, None, :]
    leading = heads_in[..., :quarter]
    trailing = heads_in[..., quarter:]
    return jnp.concatenate([leading * cosine_part - trailing * sine_part, leading * sine_part + trailing * cosine_part], axis=-1)

def grid_rotary(heads_in, positions):
    half_width = heads_in.shape[-1] // 2
    grid_row = (positions // GRID_W).astype(jnp.float32)
    grid_col = (positions % GRID_W).astype(jnp.float32)
    return jnp.concatenate([rotate_half(heads_in[..., :half_width], grid_row), rotate_half(heads_in[..., half_width:], grid_col)], axis=-1)

def reference(queries, keys, values, documents, query_gain, key_gain, residual, out_weight, norm_gain, up_weight, down_weight):
    group_size = HQ // KV
    positions = jnp.arange(TOKENS, dtype=jnp.int32)
    queries_rot = grid_rotary(head_norm(queries.reshape(TOKENS, HQ, HD), query_gain), positions).astype(jnp.bfloat16)
    keys_rot = grid_rotary(head_norm(keys.reshape(TOKENS, KV, HD), key_gain), positions).astype(jnp.bfloat16)
    key_float = keys_rot.astype(jnp.float32)
    value_float = values.reshape(TOKENS, KV, HD).astype(jnp.float32)
    query_blocks = queries_rot.reshape(N_SP, TOK_DEV, KV, group_size, HD)
    doc_blocks = documents.reshape(N_SP, TOK_DEV)

    def attend(block_pair):
        query_block, doc_block = block_pair
        scores = jnp.einsum('qkgd,skd->kgqs', query_block.astype(jnp.float32), key_float) * HD ** (-0.5)
        same_doc = doc_block[:, None] == documents[None, :]
        scores = jnp.where(same_doc, scores, masked_score)
        row_max = lax.optimization_barrier(jnp.max(scores, axis=-1, keepdims=True))
        probs = jnp.where(same_doc, jnp.exp(scores - row_max), 0.0)
        row_sum = lax.optimization_barrier(jnp.sum(probs, axis=-1))
        probs_low = lax.optimization_barrier(probs.astype(jnp.bfloat16)).astype(jnp.float32)
        summed = jnp.einsum('kgqs,skd->qkgd', probs_low, value_float)
        return (summed / jnp.transpose(row_sum, (2, 0, 1))[..., None]).astype(jnp.bfloat16)
    attended = lax.map(attend, (query_blocks, doc_blocks)).reshape(TOKENS, HQ * HD)
    head_width = HQ * HD // N_TP
    branch = jnp.zeros((TOKENS, D), jnp.float32)
    for head_block in range(N_TP):
        lower = head_block * head_width
        part_sum = jnp.dot(attended[:, lower:lower + head_width], out_weight[lower:lower + head_width], preferred_element_type=jnp.float32)
        branch = branch + lax.optimization_barrier(part_sum.astype(jnp.bfloat16)).astype(jnp.float32)
    stream = residual.astype(jnp.float32) + branch
    normed = stream * lax.rsqrt(lax.optimization_barrier(jnp.mean(stream * stream, axis=-1, keepdims=True)) + norm_eps)
    normed = (normed * norm_gain.astype(jnp.float32)).astype(jnp.bfloat16)
    hidden = jnp.dot(normed, up_weight, preferred_element_type=jnp.float32)
    positive = jnp.maximum(hidden, 0.0)
    squared = (positive * positive).astype(jnp.bfloat16)
    unit_width = FF // N_TP
    feed = jnp.zeros((TOKENS, D), jnp.float32)
    for unit_block in range(N_TP):
        lower = unit_block * unit_width
        part_sum = jnp.dot(squared[:, lower:lower + unit_width], down_weight[lower:lower + unit_width], preferred_element_type=jnp.float32)
        feed = feed + lax.optimization_barrier(part_sum.astype(jnp.bfloat16)).astype(jnp.float32)
    return (stream + feed).astype(jnp.bfloat16)
```

```python
import functools
import jax
import jax.numpy as jnp
from jax import lax
from jax.experimental import pallas as pl
from jax.experimental.pallas import tpu as pltpu
from jax.sharding import Mesh
from jax.sharding import PartitionSpec as P

D = 4096
FF = 16384
HQ = 16
KV = 8
HD = 128
GRID_W = 64
TOK = 512
HALF = 256
N = 4

norm_eps = 1e-06
rope_base = 10000.0
masked_score = -1e30

MESH = pl.DeviceIdType.MESH
VMEM = pl.BlockSpec(memory_space=pltpu.VMEM)
ANY = pl.BlockSpec(memory_space=pl.ANY)


def shifted(index, by):
    return lax.rem(index + by + N, N)


def send(src, dst, send_sem, recv_sem, device):
    copy = pltpu.make_async_remote_copy(
        src_ref=src,
        dst_ref=dst,
        send_sem=send_sem,
        recv_sem=recv_sem,
        device_id=device,
        device_id_type=MESH,
    )
    copy.start()
    return copy


def arrived(dst, send_sem, recv_sem, device):
    pltpu.make_async_remote_copy(
        src_ref=dst,
        dst_ref=dst,
        send_sem=send_sem,
        recv_sem=recv_sem,
        device_id=device,
        device_id_type=MESH,
    ).wait_recv()


class TorusGather:
    SENDS = 20

    def __init__(self, first, second, piece, start, rows, send_sems, recv_sems, base):
        self.first, self.second = first, second
        self.a, self.b = lax.axis_index(first), lax.axis_index(second)
        self.piece, self.start, self.rows = piece, start, rows
        self.send_sems, self.recv_sems, self.base = send_sems, recv_sems, base
        self.sent = []

    def order(self, j):
        return (self.a, shifted(self.a, -1), shifted(self.a, 1), shifted(self.a, 2))[j]

    def ref(self, a, b, part):
        rows = self.rows // 2
        if part is None:
            return self.piece(a, b, self.start, self.rows)
        return self.piece(a, b, self.start + part * rows, rows)

    def put(self, k, axis, by, a, b, part):
        here = self.ref(a, b, part)
        device = {axis: shifted(lax.axis_index(axis), by)}
        k += self.base
        self.sent.append(send(here, here, self.send_sems.at[k], self.recv_sems.at[k], device))

    def take(self, k, a, b, part):
        k += self.base
        arrived(self.ref(a, b, part), self.send_sems.at[k], self.recv_sems.at[k], {self.first: self.a})

    def spread(self, j):
        self.put(4 + 4 * j, self.second, 1, self.order(j), self.b, None)
        self.put(5 + 4 * j, self.second, -1, self.order(j), self.b, None)

    def begin(self):
        self.put(0, self.first, 1, self.a, self.b, None)
        self.put(1, self.first, -1, self.a, self.b, None)
        self.spread(0)

    def near(self):
        self.take(0, self.order(1), self.b, None)
        self.put(2, self.first, 1, self.order(1), self.b, 0)
        self.spread(1)
        self.take(1, self.order(2), self.b, None)
        self.put(3, self.first, -1, self.order(2), self.b, 1)
        self.spread(2)

    def far(self):
        self.take(2, self.order(3), self.b, 0)
        self.take(3, self.order(3), self.b, 1)
        self.spread(3)

    def pass_on(self, j):
        low, high = shifted(self.b, -1), shifted(self.b, 1)
        self.take(4 + 4 * j, self.order(j), low, None)
        self.put(6 + 4 * j, self.second, 1, self.order(j), low, 0)
        self.take(5 + 4 * j, self.order(j), high, None)
        self.put(7 + 4 * j, self.second, -1, self.order(j), high, 1)

    def last(self, j):
        self.take(6 + 4 * j, self.order(j), shifted(self.b, 2), 0)
        self.take(7 + 4 * j, self.order(j), shifted(self.b, 2), 1)

    def finish(self):
        for copy in self.sent:
            copy.wait_send()


class Exchange:
    SENDS = 6

    def __init__(self, axis, source, target, stage, rows, send_sems, recv_sems, base, beyond=None):
        self.axis, self.me = axis, lax.axis_index(axis)
        self.source, self.target, self.stage, self.rows = source, target, stage, rows
        self.send_sems, self.recv_sems, self.base = send_sems, recv_sems, base
        self.beyond = beyond or {}
        self.sent = []

    def put(self, k, src, dst, by, beyond=True):
        device = {self.axis: shifted(self.me, by)}
        if beyond:
            device.update(self.beyond)
        k += self.base
        self.sent.append(send(src, dst, self.send_sems.at[k], self.recv_sems.at[k], device))

    def take(self, k, dst):
        k += self.base
        arrived(dst, self.send_sems.at[k], self.recv_sems.at[k], {self.axis: self.me})

    def begin(self):
        half = self.rows // 2
        far = shifted(self.me, 2)
        self.put(2, self.source(far, 0, half), self.stage(0), 1, False)
        self.put(3, self.source(far, half, half), self.stage(1), -1, False)
        self.put(0, self.source(shifted(self.me, 1), 0, self.rows), self.target(self.me, 0, self.rows), 1)
        self.put(1, self.source(shifted(self.me, -1), 0, self.rows), self.target(self.me, 0, self.rows), -1)

    def pass_on(self):
        half = self.rows // 2
        self.take(2, self.stage(0))
        self.put(4, self.stage(0), self.target(shifted(self.me, -1), 0, half), 1)
        self.take(3, self.stage(1))
        self.put(5, self.stage(1), self.target(shifted(self.me, 1), half, half), -1)

    def last(self):
        half = self.rows // 2
        self.take(0, self.target(shifted(self.me, -1), 0, self.rows))
        self.take(1, self.target(shifted(self.me, 1), 0, self.rows))
        self.take(4, self.target(shifted(self.me, 2), 0, half))
        self.take(5, self.target(shifted(self.me, 2), half, half))

    def finish(self):
        for copy in self.sent:
            copy.wait_send()


def swapped(u):
    lane = lax.broadcasted_iota(jnp.int32, u.shape, 1)
    ahead = pltpu.roll(u, HD - HD // 4, 1)
    behind = pltpu.roll(u, HD // 4, 1)
    return jnp.where(lax.rem(lane, HD // 2) < HD // 4, ahead, behind)


def rotated(u, gain, cosine, sine):
    u = u.astype(jnp.float32)
    u = u * lax.rsqrt(jnp.mean(u * u, axis=-1, keepdims=True) + norm_eps) * gain
    return (u * cosine + swapped(u) * sine).astype(jnp.bfloat16)


def barrier_with(peers):
    barrier = pltpu.get_barrier_semaphore()
    for peer in peers:
        pl.semaphore_signal(barrier, inc=1, device_id=peer, device_id_type=MESH)
    return lambda: pl.semaphore_wait(barrier, len(peers))


def gather_kernel(
    keys, values, docs, gain, cosine, sine, out_w, up_w, down_w,
    kv, all_docs, out_cols, up_x, down_x,
    up_stage, down_stage, out_stage, send_sems, recv_sems, local_sems,
):
    z, x, y, c = (lax.axis_index(n) for n in ("z", "x", "y", "c"))
    other = 1 - c
    peers = [
        {"z": shifted(z, dz), "x": shifted(x, dx)} for dz in range(N) for dx in range(N) if dz or dx
    ] + [
        {"y": shifted(y, dy), "c": cc} for dy in range(N) for cc in (c, other) if dy or cc is other
    ]
    wait = barrier_with(peers)
    sp = z * N + x
    tp = y * 2 + c
    kv[sp, :, :HD] = rotated(keys[...], gain[...], cosine[...], sine[...])
    kv[sp, :, HD:] = values[...]
    all_docs[sp] = docs[...]
    local = [
        pltpu.make_async_copy(
            out_w.at[:, pl.ds(pl.multiple_of(tp * TOK, TOK), TOK)], out_cols.at[tp], local_sems.at[0]
        ),
        pltpu.make_async_copy(
            up_w.at[:, pl.ds(pl.multiple_of(x * TOK, TOK), TOK)], up_x.at[x], local_sems.at[1]
        ),
        pltpu.make_async_copy(
            down_w.at[pl.ds(pl.multiple_of(x * TOK, TOK), TOK), :], down_x.at[x], local_sems.at[2]
        ),
    ]
    for copy in local:
        copy.start()
    wait()

    def place(zz, xx, start, rows):
        return kv.at[zz * N + xx, pl.ds(start, rows), :]

    gathers = [
        TorusGather("x", "z", lambda a, b, s, r: place(b, a, s, r), 0, TOK, send_sems, recv_sems, 0),
    ]
    ups = Exchange(
        "x",
        lambda to, s, r: up_w.at[pl.ds(s, r), pl.ds(pl.multiple_of(to * TOK, TOK), TOK)],
        lambda who, s, r: up_x.at[who, pl.ds(s, r), :],
        lambda i: up_stage.at[i],
        256, send_sems, recv_sems, 40,
    )
    downs = Exchange(
        "x",
        lambda to, s, r: down_w.at[pl.ds(pl.multiple_of(to * TOK + s, HALF), r), :],
        lambda who, s, r: down_x.at[who, pl.ds(s, r), :],
        lambda i: down_stage.at[i],
        512, send_sems, recv_sems, 46,
    )
    outs = []
    for i, cc in enumerate((c, other)):
        def source(to, s, r, cc=cc):
            return out_w.at[pl.ds(s, r), pl.ds(pl.multiple_of((to * 2 + cc) * TOK, TOK), TOK)]

        def target(who, s, r, cc=cc):
            return out_cols.at[who * 2 + cc, pl.ds(s, r), :]

        outs.append((source, i, cc))
    exchanges = []
    for source, i, cc in outs:
        ex = Exchange(
            "y", source, None, lambda k, i=i: out_stage.at[i, k], 256, send_sems, recv_sems,
            52 + 6 * i, {"c": cc},
        )
        ex.target = lambda who, s, r: out_cols.at[who * 2 + c, pl.ds(s, r), :]
        ex.landed = lambda who, s, r, cc=cc: out_cols.at[who * 2 + cc, pl.ds(s, r), :]
        exchanges.append(ex)

    for g in gathers:
        g.begin()
    for ex in exchanges:
        ex.begin()
    twin = send(
        out_w.at[:, pl.ds(pl.multiple_of((y * 2 + other) * TOK, TOK), TOK)], out_cols.at[tp],
        send_sems.at[64], recv_sems.at[64], {"c": other},
    )
    doc_copies = []
    k = 65
    for dz in range(N):
        for dx in range(N):
            if dz or dx:
                doc_copies.append(
                    send(
                        all_docs.at[sp], all_docs.at[sp], send_sems.at[k], recv_sems.at[k],
                        {"z": shifted(z, dz), "x": shifted(x, dx)},
                    )
                )
                k += 1
    ups.begin()
    downs.begin()
    for g in gathers:
        g.near()
    for g in gathers:
        g.far()
    for ex in exchanges:
        ex.pass_on()
    for j in range(N):
        for g in gathers:
            g.pass_on(j)
        if j == 1:
            ups.pass_on()
            downs.pass_on()
    for j in range(N):
        for g in gathers:
            g.last(j)
    k = 65
    for dz in range(N):
        for dx in range(N):
            if dz or dx:
                arrived(
                    all_docs.at[shifted(z, -dz) * N + shifted(x, -dx)], send_sems.at[k], recv_sems.at[k],
                    {"z": z},
                )
                k += 1
    arrived(out_cols.at[y * 2 + other], send_sems.at[64], recv_sems.at[64], {"c": c})
    for ex in exchanges:
        ex.target, keep = ex.landed, ex.target
        ex.last()
        ex.target = keep
    ups.last()
    downs.last()
    for copy in local:
        copy.wait()
    for done in (*gathers, ups, downs, *exchanges):
        done.finish()
    twin.wait_send()
    for copy in doc_copies:
        copy.wait_send()


def gathered(keys, values, docs, gain, cosine, sine, out_w, up_w, down_w):
    bf = jnp.bfloat16
    return pl.pallas_call(
        gather_kernel,
        out_shape=(
            jax.ShapeDtypeStruct((16, TOK, 2 * HD), bf),
            jax.ShapeDtypeStruct((16, 1, TOK), jnp.int32),
            jax.ShapeDtypeStruct((8, 256, TOK), bf),
            jax.ShapeDtypeStruct((N, 256, TOK), bf),
            jax.ShapeDtypeStruct((N, TOK, 256), bf),
        ),
        in_specs=[VMEM] * 6 + [ANY] * 3,
        out_specs=(VMEM, VMEM, ANY, ANY, ANY),
        scratch_shapes=[
            pltpu.VMEM((2, 128, TOK), bf),
            pltpu.VMEM((2, 256, 256), bf),
            pltpu.VMEM((2, 2, 128, TOK), bf),
            pltpu.SemaphoreType.DMA((80,)),
            pltpu.SemaphoreType.DMA((80,)),
            pltpu.SemaphoreType.DMA((3,)),
        ],
        compiler_params=pltpu.CompilerParams(collective_id=0, has_side_effects=True, vmem_limit_bytes=40 << 20),
        name="gather_kv",
    )(keys, values, docs, gain, cosine, sine, out_w, up_w, down_w)


def attention_kernel(queries, gain, cosine, sine, own_docs, kv, docs, out):
    scale = HD ** (-0.5) * 1.4426950408889634
    everyone = docs[...]
    for t in range(TOK // HALF):
        rows = pl.ds(t * HALF, HALF)
        mine = own_docs[rows, :]
        low = jnp.sum((everyone < jnp.min(mine)).astype(jnp.int32))
        high = jnp.sum((everyone <= jnp.max(mine)).astype(jnp.int32))
        q = [
            rotated(queries[rows, h * HD : (h + 1) * HD], gain[...], cosine[rows, :], sine[rows, :])
            for h in range(2)
        ]

        def step(j, carry):
            k = kv[j, :, :HD]
            v = kv[j, :, HD:]
            same = mine == docs[j]
            after = []
            for h in range(2):
                top, total, weighted = carry[h]
                s = lax.dot_general(q[h], k, (((1,), (1,)), ((), ())), preferred_element_type=jnp.float32)
                s = jnp.where(same, s, masked_score)
                new_top = jnp.maximum(top, jnp.max(s, axis=-1, keepdims=True))
                p = jnp.exp2((s - new_top) * scale)
                fade = jnp.exp2((top - new_top) * scale)
                total = total * fade + jnp.sum(p, axis=-1, keepdims=True)
                weighted = weighted * fade + jnp.dot(
                    p.astype(jnp.bfloat16), v, preferred_element_type=jnp.float32
                )
                after.append((new_top, total, weighted))
            return tuple(after)

        start = (
            jnp.full((HALF, 1), masked_score, jnp.float32),
            jnp.zeros((HALF, 1), jnp.float32),
            jnp.zeros((HALF, HD), jnp.float32),
        )
        ends = lax.fori_loop(lax.div(low, TOK), lax.div(high + (TOK - 1), TOK), step, (start, start))
        for h in range(2):
            top, total, weighted = ends[h]
            out[rows, h * HD : (h + 1) * HD] = (weighted / total).astype(jnp.bfloat16)


def attended_heads(queries, gain, cosine, sine, own_docs, kv, docs):
    return pl.pallas_call(
        attention_kernel,
        out_shape=jax.ShapeDtypeStruct((TOK, 2 * HD), jnp.bfloat16),
        in_specs=[VMEM] * 7,
        out_specs=VMEM,
        compiler_params=pltpu.CompilerParams(vmem_limit_bytes=48 << 20),
        cost_estimate=pl.CostEstimate(flops=4 << 30, bytes_accessed=6 << 20, transcendentals=8 << 20),
        name="attend",
    )(queries, gain, cosine, sine, own_docs, kv, docs)


def tables(sp):
    position = sp * TOK + jnp.arange(TOK, dtype=jnp.int32)
    lane = jnp.arange(HD, dtype=jnp.int32)
    quarter = HD // 4
    inverse_freq = rope_base ** (-(lane % quarter).astype(jnp.float32) / quarter)
    place = jnp.where(
        lane[None, :] < HD // 2, (position // GRID_W)[:, None], (position % GRID_W)[:, None]
    ).astype(jnp.float32)
    angles = place * inverse_freq[None, :]
    sign = jnp.where(lane % (HD // 2) < quarter, -1.0, 1.0)
    return jnp.cos(angles), jnp.sin(angles) * sign[None, :]


class RingGather:
    SENDS = 4

    def __init__(self, axis, piece, own, send_sems, recv_sems, base):
        self.axis, self.me = axis, lax.axis_index(axis)
        self.piece, self.own = piece, own
        self.send_sems, self.recv_sems, self.base = send_sems, recv_sems, base
        self.sent = []

    def put(self, k, src, dst, by):
        device = {self.axis: shifted(self.me, by)}
        k += self.base
        self.sent.append(send(src, dst, self.send_sems.at[k], self.recv_sems.at[k], device))

    def take(self, k, dst):
        k += self.base
        arrived(dst, self.send_sems.at[k], self.recv_sems.at[k], {self.axis: self.me})

    def begin(self):
        self.put(0, self.own, self.piece(self.me, None), 1)
        self.put(1, self.own, self.piece(self.me, None), -1)

    def low(self):
        who = shifted(self.me, -1)
        self.take(0, self.piece(who, None))
        self.put(2, self.piece(who, 0), self.piece(who, 0), 1)

    def high(self):
        who = shifted(self.me, 1)
        self.take(1, self.piece(who, None))
        self.put(3, self.piece(who, 1), self.piece(who, 1), -1)

    def far(self):
        who = shifted(self.me, 2)
        self.take(2, self.piece(who, 0))
        self.take(3, self.piece(who, 1))

    def finish(self):
        for copy in self.sent:
            copy.wait_send()


class TorusReduce:
    SENDS = 20

    def __init__(self, first, second, piece, start, rows, bufs, send_sems, recv_sems, base):
        self.first, self.second = first, second
        self.a, self.b = lax.axis_index(first), lax.axis_index(second)
        self.piece, self.start, self.rows = piece, start, rows
        self.far_first, self.near_first, self.far_second, self.near_second = bufs
        self.send_sems, self.recv_sems, self.base = send_sems, recv_sems, base
        self.sent = []

    def dest(self, j):
        return shifted(self.b, (2, 1, -1, 0)[j])

    def ref(self, a, b, part):
        rows = self.rows // 2
        if part is None:
            return self.piece(a, b, self.start, self.rows)
        return self.piece(a, b, self.start + part * rows, rows)

    def put(self, k, axis, by, src, dst):
        device = {axis: shifted(lax.axis_index(axis), by)}
        k += self.base
        self.sent.append(send(src, dst, self.send_sems.at[k], self.recv_sems.at[k], device))

    def take(self, k, dst):
        k += self.base
        arrived(dst, self.send_sems.at[k], self.recv_sems.at[k], {self.first: self.a})

    @staticmethod
    def add(into, *others):
        total = into[...].astype(jnp.float32)
        for other in others:
            total = total + other[...].astype(jnp.float32)
        into[...] = total.astype(into.dtype)

    def far(self, j):
        a, b = shifted(self.a, 2), self.dest(j)
        self.put(4 * j, self.first, 1, self.ref(a, b, 0), self.far_first.at[0, j])
        self.put(4 * j + 1, self.first, -1, self.ref(a, b, 1), self.far_first.at[1, j])

    def up(self, j):
        a, b = shifted(self.a, 1), self.dest(j)
        self.take(4 * j, self.far_first.at[0, j])
        self.add(self.ref(a, b, 0), self.far_first.at[0, j])
        self.put(4 * j + 2, self.first, 1, self.ref(a, b, None), self.near_first.at[0, j])

    def down(self, j):
        a, b = shifted(self.a, -1), self.dest(j)
        self.take(4 * j + 1, self.far_first.at[1, j])
        self.add(self.ref(a, b, 1), self.far_first.at[1, j])
        self.put(4 * j + 3, self.first, -1, self.ref(a, b, None), self.near_first.at[1, j])

    def own(self, j):
        self.take(4 * j + 2, self.near_first.at[0, j])
        self.take(4 * j + 3, self.near_first.at[1, j])
        self.add(self.ref(self.a, self.dest(j), None), self.near_first.at[0, j], self.near_first.at[1, j])

    def second_far(self):
        b = shifted(self.b, 2)
        self.put(16, self.second, 1, self.ref(self.a, b, 0), self.far_second.at[0])
        self.put(17, self.second, -1, self.ref(self.a, b, 1), self.far_second.at[1])

    def second_up(self):
        b = shifted(self.b, 1)
        self.take(16, self.far_second.at[0])
        self.add(self.ref(self.a, b, 0), self.far_second.at[0])
        self.put(18, self.second, 1, self.ref(self.a, b, None), self.near_second.at[0])

    def second_down(self):
        b = shifted(self.b, -1)
        self.take(17, self.far_second.at[1])
        self.add(self.ref(self.a, b, 1), self.far_second.at[1])
        self.put(19, self.second, -1, self.ref(self.a, b, None), self.near_second.at[1])

    def total(self):
        self.take(18, self.near_second.at[0])
        self.take(19, self.near_second.at[1])
        total = self.ref(self.a, self.b, None)[...].astype(jnp.float32)
        total = total + self.near_second[0].astype(jnp.float32)
        return total + self.near_second[1].astype(jnp.float32)

    def finish(self):
        for copy in self.sent:
            copy.wait_send()


def layer_kernel(
    att, out_cols, residual, gains, up_x, down_x, mixed,
    x_all, up_all, down_all, sums, theirs, stream, hidden, squared, squares,
    far_first, near_first, far_second, near_second, send_sems, recv_sems, local_sems,
):
    z, x, y, c = (lax.axis_index(n) for n in ("z", "x", "y", "c"))
    other = 1 - c
    tp = y * 2 + c
    group = [{"y": shifted(y, dy), "c": cc} for dy in range(N) for cc in (c, other) if dy or cc is other]
    wait = barrier_with(
        group + [{"z": shifted(z, 1)}, {"z": shifted(z, -1)}, {"x": shifted(x, 1)}, {"x": shifted(x, -1)}]
    )

    def att_slot(t, part):
        rows = pl.ds(0, TOK) if part is None else pl.ds(part * HALF, HALF)
        return sums.at[0, lax.div(t, 4), lax.rem(t, 4), rows, pl.ds(0, 256)]

    def col_slot(t):
        return theirs.at[lax.div(t, 4), lax.rem(t, 4), pl.ds(0, 256), :]

    local = [
        pltpu.make_async_copy(out_cols.at[t], col_slot(t), local_sems.at[t]) for t in range(8)
    ]
    for copy in local:
        copy.start()
    weights = [
        pltpu.make_async_copy(up_x, up_all.at[z], local_sems.at[8]),
        pltpu.make_async_copy(down_x, down_all.at[z], local_sems.at[9]),
    ]
    for copy in weights:
        copy.start()
    wait()

    heads = RingGather("y", lambda who, part: att_slot(who * 2 + c, part), att, send_sems, recv_sems, 0)
    heads.begin()
    handed = []

    def hand(k, src, dst):
        handed.append(send(src, dst, send_sems.at[k], recv_sems.at[k], {"c": other}))

    def taken(k, dst):
        arrived(dst, send_sems.at[k], recv_sems.at[k], {"c": c})

    hand(4, att, att_slot(tp, None))

    def half_of(ref, z_at, part):
        at = ref.at[z_at]
        return at if part is None else at.at[pl.ds(2 * part, 2)]

    ups = RingGather("z", lambda who, part: half_of(up_all, who, part), up_x, send_sems, recv_sems, 8)
    downs = RingGather("z", lambda who, part: half_of(down_all, who, part), down_x, send_sems, recv_sems, 12)
    ups.begin()
    downs.begin()
    for copy in local:
        copy.wait()

    def project(t, piece):
        part = jnp.dot(piece[...], col_slot(t)[...], preferred_element_type=jnp.float32)
        stream[...] += part.astype(jnp.bfloat16).astype(jnp.float32)

    def project_slot(t):
        project(t, att_slot(t, None))

    y_low, y_high, y_far = shifted(y, -1), shifted(y, 1), shifted(y, 2)
    stream[...] = residual[...].astype(jnp.float32)
    project(tp, att)
    heads.low()
    hand(5, att_slot(y_low * 2 + c, None), att_slot(y_low * 2 + c, None))
    heads.high()
    hand(6, att_slot(y_high * 2 + c, None), att_slot(y_high * 2 + c, None))
    taken(4, att_slot(y * 2 + other, None))
    project_slot(y * 2 + other)
    project_slot(y_low * 2 + c)
    project_slot(y_high * 2 + c)
    heads.far()
    hand(7, att_slot(y_far * 2 + c, None), att_slot(y_far * 2 + c, None))
    taken(5, att_slot(y_low * 2 + other, None))
    project_slot(y_low * 2 + other)
    taken(6, att_slot(y_high * 2 + other, None))
    project_slot(y_high * 2 + other)
    project_slot(y_far * 2 + c)
    taken(7, att_slot(y_far * 2 + other, None))
    project_slot(y_far * 2 + other)

    heads.finish()
    for copy in handed:
        copy.wait_send()
    handed.clear()

    whole = stream[...]
    partial = jnp.sum(whole * whole, axis=-1, keepdims=True)
    squares[tp] = jnp.transpose(jnp.broadcast_to(partial, (TOK, HD)))[:8]
    square_copies = [
        send(squares.at[tp], squares.at[tp], send_sems.at[16 + i], recv_sems.at[16 + i], peer)
        for i, peer in enumerate(group)
    ]
    i = 0
    for dy in range(N):
        for cc in (c, other):
            if dy or cc is other:
                arrived(squares.at[shifted(y, -dy) * 2 + cc], send_sems.at[16 + i], recv_sems.at[16 + i], {"c": c})
                i += 1
    full = squares[0]
    for t in range(1, 8):
        full = full + squares[t]
    full = jnp.transpose(jnp.broadcast_to(full[:1], (HD, TOK)))
    inverse = lax.rsqrt(full[:, :1] / D + norm_eps)
    x_all[x, tp] = (stream[...] * inverse * gains[tp]).astype(jnp.bfloat16)

    def place(xx, yy, start, rows):
        return x_all.at[xx, yy * 2 + c, pl.ds(start, rows), :]

    gathers = [
        TorusGather("y", "x", lambda a, b, s, r: place(b, a, s, r), 0, HALF, send_sems, recv_sems, 24),
        TorusGather("x", "y", place, HALF, HALF, send_sems, recv_sems, 44),
    ]

    def share(g, n, j, a, b):
        ref = g.ref(a, b, None)
        hand(64 + 16 * n + j, ref, ref)

    for g in gathers:
        g.begin()
    for n, g in enumerate(gathers):
        share(g, n, 0, g.a, g.b)
    for n, g in enumerate(gathers):
        g.near()
        share(g, n, 4, g.order(1), g.b)
        share(g, n, 8, g.order(2), g.b)
    for n, g in enumerate(gathers):
        g.far()
        share(g, n, 12, g.order(3), g.b)
    for j in range(N):
        for n, g in enumerate(gathers):
            g.pass_on(j)
            share(g, n, 4 * j + 1, g.order(j), shifted(g.b, -1))
            share(g, n, 4 * j + 2, g.order(j), shifted(g.b, 1))
        if j == 1:
            ups.low()
            ups.high()
    for j in range(N):
        for n, g in enumerate(gathers):
            g.last(j)
            share(g, n, 4 * j + 3, g.order(j), shifted(g.b, 2))
    downs.low()
    downs.high()
    for n, g in enumerate(gathers):
        for j in range(N):
            for i, by in enumerate((0, -1, 1, 2)):
                a, b = g.order(j), shifted(g.b, by)
                xx, yy = (b, a) if n == 0 else (a, b)
                taken(
                    64 + 16 * n + 4 * j + i,
                    x_all.at[xx, yy * 2 + other, pl.ds(n * HALF, HALF), :],
                )
    for copy in weights:
        copy.wait()
    ups.far()
    downs.far()

    def feed(i, xx):
        hidden[...] = jnp.zeros_like(hidden)

        @pl.loop(0, 8)
        def _(t):
            w = up_all[lax.div(t, 2), pl.ds(2 * lax.rem(t, 2), 2)].reshape(TOK, TOK)
            hidden[...] += jnp.dot(x_all[xx, t], w, preferred_element_type=jnp.float32)

        positive = jnp.maximum(hidden[...], 0.0)
        squared[...] = (positive * positive).astype(jnp.bfloat16)

        @pl.loop(0, 8)
        def _(t):
            for part in range(2):
                w = down_all[lax.div(t, 2), 2 * lax.rem(t, 2) + part]
                sums[lax.rem(t, 2), xx, lax.div(t, 2), :, part * 256 : (part + 1) * 256] = jnp.dot(
                    squared[...], w, preferred_element_type=jnp.float32
                ).astype(jnp.bfloat16)

        hand(96 + i, sums.at[other, xx], theirs.at[xx])

    def joined(i, xx):
        taken(96 + i, theirs.at[xx])

        @pl.loop(0, N)
        def _(yy):
            TorusReduce.add(sums.at[c, xx, yy], theirs.at[xx, yy])

    def sum_place(xx, yy, start, rows):
        return sums.at[c, xx, yy, pl.ds(start, rows), :]

    def bufs(n):
        return far_first.at[n], near_first.at[n], far_second.at[n], near_second.at[n]

    rows_x = TorusReduce("x", "y", sum_place, 0, HALF, bufs(0), send_sems, recv_sems, 100)
    rows_y = TorusReduce(
        "y", "x", lambda a, b, s, r: sum_place(b, a, s, r), HALF, HALF, bufs(1), send_sems, recv_sems, 120
    )
    blocks = [rows_y.dest(j) for j in range(N)]
    feed(0, blocks[0])
    feed(1, blocks[1])
    joined(0, blocks[0])
    for j in range(N):
        rows_x.far(j)
    rows_y.far(0)
    feed(2, blocks[2])
    joined(1, blocks[1])
    rows_y.far(1)
    for j in range(N):
        rows_x.up(j)
    rows_y.up(0)
    rows_y.down(0)
    feed(3, blocks[3])
    joined(2, blocks[2])
    rows_y.far(2)
    for j in range(N):
        rows_x.down(j)
    rows_y.up(1)
    rows_y.down(1)
    joined(3, blocks[3])
    rows_y.far(3)
    rows_y.up(2)
    rows_y.down(2)
    rows_y.up(3)
    rows_y.down(3)
    for j in range(N):
        for r in (rows_x, rows_y):
            r.own(j)
            if j == 0:
                r.second_far()
            if j == 1:
                r.second_up()
            if j == 2:
                r.second_down()
    mixed[:HALF, :] = (stream[:HALF, :] + rows_x.total()).astype(jnp.bfloat16)
    mixed[HALF:, :] = (stream[HALF:, :] + rows_y.total()).astype(jnp.bfloat16)
    for done in (ups, downs, *gathers, rows_x, rows_y):
        done.finish()
    for copy in (*handed, *square_copies):
        copy.wait_send()


def layer(att, out_cols, residual, gains, up_x, down_x):
    bf = jnp.bfloat16
    return pl.pallas_call(
        layer_kernel,
        out_shape=jax.ShapeDtypeStruct((TOK, TOK), bf),
        in_specs=[VMEM, ANY, VMEM, VMEM, ANY, ANY],
        out_specs=VMEM,
        scratch_shapes=[
            pltpu.VMEM((N, 8, TOK, TOK), bf),
            pltpu.VMEM((N, N, 256, TOK), bf),
            pltpu.VMEM((N, N, TOK, 256), bf),
            pltpu.VMEM((2, N, N, TOK, TOK), bf),
            pltpu.VMEM((N, N, TOK, TOK), bf),
            pltpu.VMEM((TOK, TOK), jnp.float32),
            pltpu.VMEM((TOK, TOK), jnp.float32),
            pltpu.VMEM((TOK, TOK), bf),
            pltpu.VMEM((8, 8, TOK), jnp.float32),
            pltpu.VMEM((2, 2, N, 128, TOK), bf),
            pltpu.VMEM((2, 2, N, HALF, TOK), bf),
            pltpu.VMEM((2, 2, 128, TOK), bf),
            pltpu.VMEM((2, 2, HALF, TOK), bf),
            pltpu.SemaphoreType.DMA((140,)),
            pltpu.SemaphoreType.DMA((140,)),
            pltpu.SemaphoreType.DMA((10,)),
        ],
        compiler_params=pltpu.CompilerParams(
            collective_id=1, has_side_effects=True, vmem_limit_bytes=67043328
        ),
        name="layer",
    )(att, out_cols, residual, gains, up_x, down_x)


def body(
    queries, keys, values, documents, query_gain, key_gain, residual, out_weight, norm_gain, up_weight, down_weight
):
    cosine, sine = tables(lax.axis_index(("z", "x")))
    kv, docs, out_cols, up_x, down_x = gathered(
        keys, values, documents.reshape(1, TOK), key_gain.reshape(1, HD), cosine, sine,
        out_weight, up_weight, down_weight,
    )
    att = attended_heads(
        queries, query_gain.reshape(1, HD), cosine, sine, documents.reshape(TOK, 1), kv, docs
    )
    return layer(att, out_cols, residual, norm_gain.reshape(8, 1, TOK), up_x, down_x)


def solution(mesh):
    split = Mesh(mesh.devices.reshape(N, N, N, 2), ("z", "x", "y", "c"))
    sp, tp = ("z", "x"), ("y", "c")
    return jax.shard_map(
        body,
        mesh=split,
        in_specs=(
            P(sp, tp), P(sp, tp), P(sp, tp), P(sp), P(), P(), P(sp, tp), P(tp, None), P(), P(sp, tp), P(tp, sp),
        ),
        out_specs=P(sp, tp),
        check_vma=False,
    )
```

```python
import functools
import jax
import jax.numpy as jnp
from jax import lax
from jax.experimental import pallas as pl
from jax.experimental.pallas import tpu as pltpu
from jax.sharding import Mesh
from jax.sharding import PartitionSpec as P

D = 4096
FF = 16384
HQ = 16
KV = 8
HD = 128
GRID_W = 64
TOK = 512
HALF = 256
N = 4

norm_eps = 1e-06
rope_base = 10000.0
masked_score = -1e30
query_mark = 128.0
key_mark = 96.0

MESH = pl.DeviceIdType.MESH
VMEM = pl.BlockSpec(memory_space=pltpu.VMEM)
ANY = pl.BlockSpec(memory_space=pl.ANY)


def shifted(index, by):
    return lax.rem(index + by + N, N)


def send(src, dst, send_sem, recv_sem, device):
    copy = pltpu.make_async_remote_copy(
        src_ref=src,
        dst_ref=dst,
        send_sem=send_sem,
        recv_sem=recv_sem,
        device_id=device,
        device_id_type=MESH,
    )
    copy.start()
    return copy


def arrived(dst, send_sem, recv_sem, device):
    pltpu.make_async_remote_copy(
        src_ref=dst,
        dst_ref=dst,
        send_sem=send_sem,
        recv_sem=recv_sem,
        device_id=device,
        device_id_type=MESH,
    ).wait_recv()


class TorusGather:
    SENDS = 20

    def __init__(self, first, second, piece, start, rows, send_sems, recv_sems, base):
        self.first, self.second = first, second
        self.a, self.b = lax.axis_index(first), lax.axis_index(second)
        self.piece, self.start, self.rows = piece, start, rows
        self.send_sems, self.recv_sems, self.base = send_sems, recv_sems, base
        self.sent = []

    def order(self, j):
        return (self.a, shifted(self.a, -1), shifted(self.a, 1), shifted(self.a, 2))[j]

    def ref(self, a, b, part):
        rows = self.rows // 2
        if part is None:
            return self.piece(a, b, self.start, self.rows)
        return self.piece(a, b, self.start + part * rows, rows)

    def put(self, k, axis, by, a, b, part):
        here = self.ref(a, b, part)
        device = {axis: shifted(lax.axis_index(axis), by)}
        k += self.base
        self.sent.append(send(here, here, self.send_sems.at[k], self.recv_sems.at[k], device))

    def take(self, k, a, b, part):
        k += self.base
        arrived(self.ref(a, b, part), self.send_sems.at[k], self.recv_sems.at[k], {self.first: self.a})

    def spread(self, j):
        self.put(4 + 4 * j, self.second, 1, self.order(j), self.b, None)
        self.put(5 + 4 * j, self.second, -1, self.order(j), self.b, None)

    def begin(self):
        self.put(0, self.first, 1, self.a, self.b, None)
        self.put(1, self.first, -1, self.a, self.b, None)
        self.spread(0)

    def near(self):
        self.take(0, self.order(1), self.b, None)
        self.put(2, self.first, 1, self.order(1), self.b, 0)
        self.spread(1)
        self.take(1, self.order(2), self.b, None)
        self.put(3, self.first, -1, self.order(2), self.b, 1)
        self.spread(2)

    def far(self):
        self.take(2, self.order(3), self.b, 0)
        self.take(3, self.order(3), self.b, 1)
        self.spread(3)

    def pass_on(self, j):
        low, high = shifted(self.b, -1), shifted(self.b, 1)
        self.take(4 + 4 * j, self.order(j), low, None)
        self.put(6 + 4 * j, self.second, 1, self.order(j), low, 0)
        self.take(5 + 4 * j, self.order(j), high, None)
        self.put(7 + 4 * j, self.second, -1, self.order(j), high, 1)

    def last(self, j):
        self.take(6 + 4 * j, self.order(j), shifted(self.b, 2), 0)
        self.take(7 + 4 * j, self.order(j), shifted(self.b, 2), 1)

    def finish(self):
        for copy in self.sent:
            copy.wait_send()


class Exchange:
    SENDS = 6

    def __init__(self, axis, source, target, stage, rows, send_sems, recv_sems, base, beyond=None):
        self.axis, self.me = axis, lax.axis_index(axis)
        self.source, self.target, self.stage, self.rows = source, target, stage, rows
        self.send_sems, self.recv_sems, self.base = send_sems, recv_sems, base
        self.beyond = beyond or {}
        self.sent = []

    def put(self, k, src, dst, by, beyond=True):
        device = {self.axis: shifted(self.me, by)}
        if beyond:
            device.update(self.beyond)
        k += self.base
        self.sent.append(send(src, dst, self.send_sems.at[k], self.recv_sems.at[k], device))

    def take(self, k, dst):
        k += self.base
        arrived(dst, self.send_sems.at[k], self.recv_sems.at[k], {self.axis: self.me})

    def begin(self):
        half = self.rows // 2
        far = shifted(self.me, 2)
        self.put(2, self.source(far, 0, half), self.stage(0), 1, False)
        self.put(3, self.source(far, half, half), self.stage(1), -1, False)
        self.put(0, self.source(shifted(self.me, 1), 0, self.rows), self.target(self.me, 0, self.rows), 1)
        self.put(1, self.source(shifted(self.me, -1), 0, self.rows), self.target(self.me, 0, self.rows), -1)

    def pass_on(self):
        half = self.rows // 2
        self.take(2, self.stage(0))
        self.put(4, self.stage(0), self.target(shifted(self.me, -1), 0, half), 1)
        self.take(3, self.stage(1))
        self.put(5, self.stage(1), self.target(shifted(self.me, 1), half, half), -1)

    def last(self):
        half = self.rows // 2
        self.take(0, self.target(shifted(self.me, -1), 0, self.rows))
        self.take(1, self.target(shifted(self.me, 1), 0, self.rows))
        self.take(4, self.target(shifted(self.me, 2), 0, half))
        self.take(5, self.target(shifted(self.me, 2), half, half))

    def finish(self):
        for copy in self.sent:
            copy.wait_send()


def swapped(u):
    lane = lax.broadcasted_iota(jnp.int32, u.shape, 1)
    ahead = pltpu.roll(u, HD - HD // 4, 1)
    behind = pltpu.roll(u, HD // 4, 1)
    return jnp.where(lax.rem(lane, HD // 2) < HD // 4, ahead, behind)


def rotated(u, gain, cosine, sine):
    u = u.astype(jnp.float32)
    u = u * lax.rsqrt(jnp.mean(u * u, axis=-1, keepdims=True) + norm_eps) * gain
    return (u * cosine + swapped(u) * sine).astype(jnp.bfloat16)


def barrier_with(peers):
    barrier = pltpu.get_barrier_semaphore()
    for peer in peers:
        pl.semaphore_signal(barrier, inc=1, device_id=peer, device_id_type=MESH)
    return lambda: pl.semaphore_wait(barrier, len(peers))


def tables(sp):
    position = sp * TOK + jnp.arange(TOK, dtype=jnp.int32)
    lane = jnp.arange(HD, dtype=jnp.int32)
    quarter = HD // 4
    inverse_freq = rope_base ** (-(lane % quarter).astype(jnp.float32) / quarter)
    place = jnp.where(
        lane[None, :] < HD // 2, (position // GRID_W)[:, None], (position % GRID_W)[:, None]
    ).astype(jnp.float32)
    angles = place * inverse_freq[None, :]
    sign = jnp.where(lane % (HD // 2) < quarter, -1.0, 1.0)
    return jnp.cos(angles), jnp.sin(angles) * sign[None, :]


class RingGather:
    SENDS = 4

    def __init__(self, axis, piece, own, send_sems, recv_sems, base):
        self.axis, self.me = axis, lax.axis_index(axis)
        self.piece, self.own = piece, own
        self.send_sems, self.recv_sems, self.base = send_sems, recv_sems, base
        self.sent = []

    def put(self, k, src, dst, by):
        device = {self.axis: shifted(self.me, by)}
        k += self.base
        self.sent.append(send(src, dst, self.send_sems.at[k], self.recv_sems.at[k], device))

    def take(self, k, dst):
        k += self.base
        arrived(dst, self.send_sems.at[k], self.recv_sems.at[k], {self.axis: self.me})

    def begin(self):
        self.put(0, self.own, self.piece(self.me, None), 1)
        self.put(1, self.own, self.piece(self.me, None), -1)

    def low(self):
        who = shifted(self.me, -1)
        self.take(0, self.piece(who, None))
        self.put(2, self.piece(who, 0), self.piece(who, 0), 1)

    def high(self):
        who = shifted(self.me, 1)
        self.take(1, self.piece(who, None))
        self.put(3, self.piece(who, 1), self.piece(who, 1), -1)

    def far(self):
        who = shifted(self.me, 2)
        self.take(2, self.piece(who, 0))
        self.take(3, self.piece(who, 1))

    def finish(self):
        for copy in self.sent:
            copy.wait_send()


class TorusReduce:
    SENDS = 20

    def __init__(self, first, second, piece, start, rows, bufs, send_sems, recv_sems, base):
        self.first, self.second = first, second
        self.a, self.b = lax.axis_index(first), lax.axis_index(second)
        self.piece, self.start, self.rows = piece, start, rows
        self.buf = bufs
        self.send_sems, self.recv_sems, self.base = send_sems, recv_sems, base
        self.sent = []

    def dest(self, j):
        return shifted(self.b, (2, 1, -1, 0)[j])

    def ref(self, a, b, part):
        rows = self.rows // 2
        if part is None:
            return self.piece(a, b, self.start, self.rows)
        return self.piece(a, b, self.start + part * rows, rows)

    def put(self, k, axis, by, src, dst):
        device = {axis: shifted(lax.axis_index(axis), by)}
        k += self.base
        self.sent.append(send(src, dst, self.send_sems.at[k], self.recv_sems.at[k], device))

    def take(self, k, dst):
        k += self.base
        arrived(dst, self.send_sems.at[k], self.recv_sems.at[k], {self.first: self.a})

    @staticmethod
    def add(into, *others):
        total = into[...].astype(jnp.float32)
        for other in others:
            total = total + other[...].astype(jnp.float32)
        into[...] = total.astype(into.dtype)

    def far(self, j):
        a, b = shifted(self.a, 2), self.dest(j)
        self.put(4 * j, self.first, 1, self.ref(a, b, 0), self.buf("far_first", 0, j))
        self.put(4 * j + 1, self.first, -1, self.ref(a, b, 1), self.buf("far_first", 1, j))

    def up(self, j):
        a, b = shifted(self.a, 1), self.dest(j)
        self.take(4 * j, self.buf("far_first", 0, j))
        self.add(self.ref(a, b, 0), self.buf("far_first", 0, j))
        self.put(4 * j + 2, self.first, 1, self.ref(a, b, None), self.buf("near_first", 0, j))

    def down(self, j):
        a, b = shifted(self.a, -1), self.dest(j)
        self.take(4 * j + 1, self.buf("far_first", 1, j))
        self.add(self.ref(a, b, 1), self.buf("far_first", 1, j))
        self.put(4 * j + 3, self.first, -1, self.ref(a, b, None), self.buf("near_first", 1, j))

    def own(self, j):
        self.take(4 * j + 2, self.buf("near_first", 0, j))
        self.take(4 * j + 3, self.buf("near_first", 1, j))
        self.add(self.ref(self.a, self.dest(j), None), self.buf("near_first", 0, j), self.buf("near_first", 1, j))

    def second_far(self):
        b = shifted(self.b, 2)
        self.put(16, self.second, 1, self.ref(self.a, b, 0), self.buf("far_second", 0, 0))
        self.put(17, self.second, -1, self.ref(self.a, b, 1), self.buf("far_second", 1, 0))

    def second_up(self):
        b = shifted(self.b, 1)
        self.take(16, self.buf("far_second", 0, 0))
        self.add(self.ref(self.a, b, 0), self.buf("far_second", 0, 0))
        self.put(18, self.second, 1, self.ref(self.a, b, None), self.buf("near_second", 0, 0))

    def second_down(self):
        b = shifted(self.b, -1)
        self.take(17, self.buf("far_second", 1, 0))
        self.add(self.ref(self.a, b, 1), self.buf("far_second", 1, 0))
        self.put(19, self.second, -1, self.ref(self.a, b, None), self.buf("near_second", 1, 0))

    def total(self):
        self.take(18, self.buf("near_second", 0, 0))
        self.take(19, self.buf("near_second", 1, 0))
        total = self.ref(self.a, self.b, None)[...].astype(jnp.float32)
        total = total + self.buf("near_second", 0, 0)[...].astype(jnp.float32)
        return total + self.buf("near_second", 1, 0)[...].astype(jnp.float32)

    def finish(self):
        for copy in self.sent:
            copy.wait_send()


def layer_kernel(
    queries, keys, values, documents, query_gain, key_gain, cosines, sines,
    out_w, residuals, norm_gains, up_w, down_w, mixed,
    x_all, up_all, down_all, sums, theirs, stream, hidden, squared, squares,
    hidden_early, docs, doc_column, q_gain, k_gain, gains, send_sems, recv_sems, local_sems, free_sem,
):
    z, x, y, c = (lax.axis_index(n) for n in ("z", "x", "y", "c"))
    other = 1 - c
    sp = z * N + x
    tp = y * 2 + c
    plane = [
        {"z": shifted(z, dz), "x": shifted(x, dx)} for dz in range(N) for dx in range(N) if dz or dx
    ]
    group = [{"y": shifted(y, dy), "c": cc} for dy in range(N) for cc in (c, other) if dy or cc is other]
    wait = barrier_with(plane + group)

    def kv_place(zz, xx, start, rows):
        return sums.at[1, zz, xx, pl.ds(start, rows), :]

    def att_slot(t, part):
        rows = pl.ds(0, TOK) if part is None else pl.ds(part * HALF, HALF)
        return sums.at[0, lax.div(t, 4), lax.rem(t, 4), rows, pl.ds(0, 256)]

    def col_slot(t, start=0, rows=256):
        return theirs.at[lax.div(t, 4), lax.rem(t, 4), pl.ds(start, rows), :]

    def thousand(index):
        return pl.ds(pl.multiple_of(index * TOK, TOK), TOK)

    q_in = theirs.at[2, 0, :, pl.ds(0, 2 * HD)]
    k_in = theirs.at[2, 1, :, pl.ds(0, HD)]
    v_in = theirs.at[2, 2, :, pl.ds(0, HD)]
    q_rot = theirs.at[2, 3]
    residual = theirs.at[3, 0]
    cosine = stream.at[:, pl.ds(2 * HD, HD)]
    sine = stream.at[:, pl.ds(3 * HD, HD)]

    def local(i, src, dst):
        copy = pltpu.make_async_copy(src, dst, local_sems.at[i])
        copy.start()
        return copy

    first = [
        local(0, keys, k_in),
        local(1, values, v_in),
        local(2, cosines, cosine),
        local(3, sines, sine),
        local(4, key_gain, k_gain),
        local(5, documents, docs.at[sp]),
    ]
    second = [local(6, queries, q_in), local(7, query_gain, q_gain)]
    third = [
        local(8, residuals, residual),
        local(9, norm_gains, gains),
        local(10, out_w.at[:, thousand(tp)], col_slot(tp)),
    ]
    fourth = [
        local(11, up_w.at[:, thousand(x)], up_all.at[z, x]),
        local(12, down_w.at[thousand(x), :], down_all.at[z, x]),
    ]
    for copy in first:
        copy.wait()
    mine = kv_place(z, x, 0, 2 * HD)
    turned = jnp.transpose(rotated(k_in[...], k_gain[...], cosine[...], sine[...]).astype(jnp.float32))
    mine[HD:, :] = turned.astype(jnp.bfloat16)
    for i in range(TOK // HD):
        mine[:HD, i * HD : (i + 1) * HD] = v_in[i * HD : (i + 1) * HD, :]

    def mark(zz, xx):
        row = lax.broadcasted_iota(jnp.int32, (HD, TOK), 0)
        hot = jnp.where(row == docs[zz * N + xx], key_mark, 0.0)
        sums[1, zz, xx, 2 * HD : 3 * HD, :] = hot.astype(jnp.bfloat16)

    mark(z, x)
    column = jnp.broadcast_to(docs[sp].astype(jnp.float32), (HD, TOK))
    doc_column[...] = jnp.transpose(column).astype(jnp.int32)
    wait()

    kvs = TorusGather("x", "z", lambda a, b, s, r: kv_place(b, a, s, r), 0, 2 * HD, send_sems, recv_sems, 0)
    ups_across = Exchange(
        "x",
        lambda to, s, r: up_w.at[pl.ds(s, r), thousand(to)],
        lambda who, s, r: up_all.at[z, who, pl.ds(s, r), :],
        lambda i: squared.at[0, pl.ds(128 * i, 128), :],
        256, send_sems, recv_sems, 20,
    )
    downs_across = Exchange(
        "x",
        lambda to, s, r: down_w.at[pl.ds(pl.multiple_of(to * TOK + s, HALF), r), :],
        lambda who, s, r: down_all.at[z, who, pl.ds(s, r), :],
        lambda i: squared.at[1, pl.ds(256 * i, 256), pl.ds(0, 256)],
        512, send_sems, recv_sems, 26,
    )
    columns = []
    for i, cc in enumerate((c, other)):
        ex = Exchange(
            "y",
            lambda to, s, r, cc=cc: out_w.at[pl.ds(s, r), thousand(to * 2 + cc)],
            lambda who, s, r: col_slot(who * 2 + c, s, r),
            lambda k, i=i: squared.at[2, pl.ds(128 * (2 * i + k), 128), :],
            256, send_sems, recv_sems, 32 + 6 * i, {"c": cc},
        )
        ex.landed = lambda who, s, r, cc=cc: col_slot(who * 2 + cc, s, r)
        columns.append(ex)
    kvs.begin()
    doc_copies = [
        send(docs.at[sp], docs.at[sp], send_sems.at[45 + i], recv_sems.at[45 + i], peer)
        for i, peer in enumerate(plane)
    ]
    for ex in columns:
        ex.begin()
    twin = send(
        out_w.at[:, thousand(y * 2 + other)], col_slot(tp), send_sems.at[44], recv_sems.at[44], {"c": other}
    )

    for copy in second:
        copy.wait()
    lane = lax.broadcasted_iota(jnp.int32, (TOK, HD), 1)
    hot = jnp.where(lane == doc_column[...], query_mark, 0.0).astype(jnp.bfloat16)
    for h in range(2):
        turn = rotated(q_in[:, h * HD : (h + 1) * HD], q_gain[...], cosine[...], sine[...])
        for t in range(2):
            rows, part = slice(h * HALF, (h + 1) * HALF), slice(t * HALF, (t + 1) * HALF)
            q_rot[rows, 2 * t * HD : (2 * t + 1) * HD] = turn[part]
            q_rot[rows, (2 * t + 1) * HD : (2 * t + 2) * HD] = hot[part]
    hidden[:, :HD] = jnp.zeros((2 * TOK, HD), jnp.float32)
    hidden[:, HD : 2 * HD] = jnp.full((2 * TOK, HD), masked_score, jnp.float32)
    hidden[:, 2 * HD : 3 * HD] = jnp.zeros((2 * TOK, HD), jnp.float32)
    scale = HD ** (-0.5) * 1.4426950408889634

    def attend(count, which):
        @pl.loop(0, 2)
        def _(t):
            rows = pl.ds(pl.multiple_of(t * TOK, TOK), TOK)
            q = q_rot[:, pl.ds(pl.multiple_of(t * HALF, HALF), HALF)]
            cuts = [slice(i * HD, (i + 1) * HD) for i in range(4)]

            def step(i, carry):
                top, total, weighted = carry
                zz, xx = which(i)
                packed = sums[1, zz, xx, :HD, :]
                v = jnp.concatenate([packed[:, cut] for cut in cuts], axis=0)
                s = jnp.dot(q, sums[1, zz, xx, HD : 3 * HD, :], preferred_element_type=jnp.float32)
                s = [s[:, cut] for cut in cuts]
                most = jnp.maximum(jnp.maximum(s[0], s[1]), jnp.maximum(s[2], s[3]))
                new_top = jnp.maximum(top, jnp.max(most, axis=-1, keepdims=True))
                p = [jnp.exp2((part - new_top) * scale) for part in s]
                fade = jnp.exp2((top - new_top) * scale)
                total = total * fade + ((p[0] + p[1]) + (p[2] + p[3]))
                low = jnp.concatenate([part.astype(jnp.bfloat16) for part in p], axis=1)
                weighted = weighted * fade + jnp.dot(low, v, preferred_element_type=jnp.float32)
                return new_top, total, weighted

            start = (hidden[rows, cuts[1]], hidden[rows, cuts[2]], hidden[rows, cuts[0]])
            top, total, weighted = lax.fori_loop(0, count, step, start)
            hidden[rows, cuts[1]] = top
            hidden[rows, cuts[2]] = total
            hidden[rows, cuts[0]] = weighted

    attend(1, lambda i: (z, x))
    kvs.near()
    kvs.far()
    ups_across.begin()
    downs_across.begin()
    for i, peer in enumerate(plane):
        dz, dx = divmod(i + 1, N)
        arrived(
            docs.at[shifted(z, -dz) * N + shifted(x, -dx)], send_sems.at[45 + i], recv_sems.at[45 + i], {"z": z}
        )

    @pl.loop(1, 16)
    def _(i):
        mark(lax.rem(z + lax.div(i, N), N), lax.rem(x + i, N))

    attend(3, lambda i: (z, lax.rem(x + 1 + i, N)))
    kvs.pass_on(0)
    kvs.pass_on(1)
    for ex in columns:
        ex.pass_on()
    attend(4, lambda i: (lax.rem(z + 1 + 2 * lax.rem(i, 2), N), lax.rem(x + N - lax.div(i, 2), N)))
    kvs.pass_on(2)
    kvs.pass_on(3)
    ups_across.pass_on()
    downs_across.pass_on()
    attend(4, lambda i: (lax.rem(z + 1 + 2 * lax.rem(i, 2), N), lax.rem(x + 1 + lax.div(i, 2), N)))
    kvs.last(0)
    kvs.last(1)
    attend(2, lambda i: (lax.rem(z + 2, N), lax.rem(x + N - i, N)))
    kvs.last(2)
    kvs.last(3)
    def half_of(ref, z_at, part):
        at = ref.at[z_at]
        return at if part is None else at.at[pl.ds(2 * part, 2)]

    ups = RingGather(
        "z", lambda who, part: half_of(up_all, who, part), up_all.at[z], send_sems, recv_sems, 68
    )
    downs = RingGather(
        "z", lambda who, part: half_of(down_all, who, part), down_all.at[z], send_sems, recv_sems, 72
    )
    for copy in fourth:
        copy.wait()
    ups_across.last()
    ups.begin()
    attend(2, lambda i: (lax.rem(z + 2, N), lax.rem(x + 1 + i, N)))

    att = att_slot(tp, None)
    for t in range(2):
        for h in range(2):
            rows = slice(t * TOK + h * HALF, t * TOK + (h + 1) * HALF)
            total = jnp.sum(hidden[rows, 2 * HD : 3 * HD], axis=-1, keepdims=True)
            att[t * HALF : (t + 1) * HALF, h * HD : (h + 1) * HD] = (hidden[rows, :HD] / total).astype(jnp.bfloat16)

    handed = []

    def hand(k, src, dst):
        handed.append(send(src, dst, send_sems.at[k], recv_sems.at[k], {"c": other}))

    def taken(k, dst):
        arrived(dst, send_sems.at[k], recv_sems.at[k], {"c": c})

    heads = RingGather("y", lambda who, part: att_slot(who * 2 + c, part), att, send_sems, recv_sems, 60)
    heads.begin()
    hand(64, att, att)

    for copy in third:
        copy.wait()
    for ex in columns:
        ex.target = ex.landed
        ex.last()
    arrived(col_slot(y * 2 + other), send_sems.at[44], recv_sems.at[44], {"c": c})

    def project(t):
        part = jnp.dot(att_slot(t, None)[...], col_slot(t)[...], preferred_element_type=jnp.float32)
        stream[...] += part.astype(jnp.bfloat16).astype(jnp.float32)

    y_low, y_high, y_far = shifted(y, -1), shifted(y, 1), shifted(y, 2)
    stream[...] = residual[...].astype(jnp.float32)
    project(tp)
    heads.low()
    hand(65, att_slot(y_low * 2 + c, None), att_slot(y_low * 2 + c, None))
    heads.high()
    hand(66, att_slot(y_high * 2 + c, None), att_slot(y_high * 2 + c, None))
    taken(64, att_slot(y * 2 + other, None))
    project(y * 2 + other)
    project(y_low * 2 + c)
    project(y_high * 2 + c)
    heads.far()
    hand(67, att_slot(y_far * 2 + c, None), att_slot(y_far * 2 + c, None))
    taken(65, att_slot(y_low * 2 + other, None))
    project(y_low * 2 + other)
    taken(66, att_slot(y_high * 2 + other, None))
    project(y_high * 2 + other)
    project(y_far * 2 + c)
    taken(67, att_slot(y_far * 2 + other, None))
    project(y_far * 2 + other)

    whole = stream[...]
    partial = jnp.sum(whole * whole, axis=-1, keepdims=True)
    squares[tp] = jnp.transpose(jnp.broadcast_to(partial, (TOK, HD)))[:8]
    square_copies = [
        send(squares.at[tp], squares.at[tp], send_sems.at[76 + i], recv_sems.at[76 + i], peer)
        for i, peer in enumerate(group)
    ]
    downs_across.last()
    for done in (heads, kvs, ups_across, downs_across, *columns):
        done.finish()
    for copy in (*handed, *doc_copies, twin):
        copy.wait_send()
    handed.clear()
    i = 0
    for dy in range(N):
        for cc in (c, other):
            if dy or cc is other:
                arrived(squares.at[shifted(y, -dy) * 2 + cc], send_sems.at[76 + i], recv_sems.at[76 + i], {"c": c})
                i += 1
    full = squares[0]
    for t in range(1, 8):
        full = full + squares[t]
    full = jnp.transpose(jnp.broadcast_to(full[:1], (HD, TOK)))
    inverse = lax.rsqrt(full[:, :1] / D + norm_eps)
    x_all[x, tp] = (stream[...] * inverse * gains[tp]).astype(jnp.bfloat16)

    def place(xx, yy, start, rows):
        return x_all.at[xx, yy * 2 + c, pl.ds(start, rows), :]

    gathers = [
        TorusGather("y", "x", lambda a, b, s, r: place(b, a, s, r), 0, HALF, send_sems, recv_sems, 83),
        TorusGather("x", "y", place, HALF, HALF, send_sems, recv_sems, 103),
    ]

    def share(n, j, i):
        g = gathers[n]
        ref = g.ref(g.order(j), shifted(g.b, (0, -1, 1, 2)[i]), None)
        hand(123 + 16 * n + 4 * j + i, ref, ref)

    def shared(n, j, i):
        g = gathers[n]
        a, b = g.order(j), shifted(g.b, (0, -1, 1, 2)[i])
        xx, yy = (b, a) if n == 0 else (a, b)
        taken(123 + 16 * n + 4 * j + i, x_all.at[xx, yy * 2 + other, pl.ds(n * HALF, HALF), :])

    def weight(t):
        return up_all[lax.div(t, 2), pl.ds(2 * lax.rem(t, 2), 2)].reshape(TOK, TOK)

    def square(value):
        positive = jnp.maximum(value, 0.0)
        return (positive * positive).astype(jnp.bfloat16)

    def early(blocks, first, count, step, clear, store):
        rows = HALF * len(blocks)
        acc = hidden_early.at[pl.ds(0, rows)]
        if clear:
            acc[...] = jnp.zeros_like(acc)

        @pl.loop(0, count)
        def _(i):
            t = lax.rem(first + step * i, 8)
            parts = [x_all[xx, t, :HALF, :] for xx in blocks]
            part = parts[0] if len(parts) == 1 else jnp.concatenate(parts, axis=0)
            acc[...] += jnp.dot(part, weight(t), preferred_element_type=jnp.float32)

        if store:
            for i, xx in enumerate(blocks):
                squared[xx, :HALF, :] = square(hidden_early[i * HALF : (i + 1) * HALF, :])

    def late(first, count, step):
        @pl.loop(0, count)
        def _(i):
            t = lax.rem(first + step * i, 8)
            rows = x_all[:, t, HALF:, :].reshape(N * HALF, TOK)
            hidden[...] += jnp.dot(rows, weight(t), preferred_element_type=jnp.float32)

    for g in gathers:
        g.begin()
    for n in range(2):
        share(n, 0, 0)
    hidden[...] = jnp.zeros_like(hidden)
    for n, g in enumerate(gathers):
        g.near()
        share(n, 1, 0)
        share(n, 2, 0)
    ups.low()
    ups.high()
    downs.begin()
    for n, g in enumerate(gathers):
        g.far()
        share(n, 3, 0)
    ups.far()
    for j in range(N):
        for n in range(2):
            shared(n, j, 0)
    early([x], 0, 8, 1, True, True)
    for j in range(N):
        for n, g in enumerate(gathers):
            g.pass_on(j)
            share(n, j, 1)
            share(n, j, 2)
    late(2 * (y + 3) + c, 3, 2)
    late(2 * y + other, 1, 2)
    for j in range(N):
        for i in (1, 2):
            for n in range(2):
                shared(n, j, i)
    late(2 * (y + 3) + other, 2, 4)
    sides = [shifted(x, -1), shifted(x, 1)]
    early(sides, 0, 4, 1, True, False)
    for j in range(2):
        for n, g in enumerate(gathers):
            g.last(j)
            share(n, j, 3)
    early(sides, 4, 4, 1, False, True)
    for j in range(2, N):
        for n, g in enumerate(gathers):
            g.last(j)
            share(n, j, 3)
    downs.low()
    downs.high()
    opposite = [shifted(x, 2)]
    late(2 * (y + 2) + c, 1, 2)
    early(opposite, c, 4, 2, True, False)
    for j in range(N):
        for n in range(2):
            shared(n, j, 3)
    early(opposite, other, 4, 2, False, True)
    late(2 * (y + 2) + other, 1, 2)
    for g in gathers:
        g.finish()
    for copy in handed:
        copy.wait_send()
    handed.clear()
    for peer in ({"x": shifted(x, 1)}, {"x": shifted(x, -1)}, {"y": shifted(y, 1)}, {"y": shifted(y, -1)}):
        pl.semaphore_signal(free_sem, inc=1, device_id=peer, device_id_type=MESH)

    @pl.loop(0, N)
    def _(xx):
        rows = pl.ds(pl.multiple_of(xx * HALF, HALF), HALF)
        squared[xx, HALF:, :] = square(hidden[rows, :])

    downs.far()

    def feed(i, xx):
        def columns_of(cc):
            @pl.loop(0, N)
            def _(yy):
                pair = [down_all[yy, 2 * cc + part] for part in range(2)]
                sums[cc, xx, yy] = jnp.dot(
                    squared[xx], jnp.concatenate(pair, axis=1), preferred_element_type=jnp.float32
                ).astype(jnp.bfloat16)

        columns_of(other)
        hand(155 + i, sums.at[other, xx], theirs.at[xx])
        columns_of(c)

    def joined(i, xx):
        taken(155 + i, theirs.at[xx])

        @pl.loop(0, N)
        def _(yy):
            TorusReduce.add(sums.at[c, xx, yy], theirs.at[xx, yy])

    def sum_place(xx, yy, start, rows):
        return sums.at[c, xx, yy, pl.ds(start, rows), :]

    def bufs(n):
        def buf(kind, way, j):
            if kind == "near_first":
                return x_all.at[n, 4 * way + j, pl.ds(0, HALF), :]
            if kind == "far_first":
                return x_all.at[n, 4 * way + j, pl.ds(HALF, HALF // 2), :]
            if kind == "near_second":
                return x_all.at[2, 2 * n + way, pl.ds(0, HALF), :]
            return x_all.at[2, 2 * n + way, pl.ds(HALF, HALF // 2), :]

        return buf

    rows_x = TorusReduce("x", "y", sum_place, 0, HALF, bufs(0), send_sems, recv_sems, 159)
    rows_y = TorusReduce(
        "y", "x", lambda a, b, s, r: sum_place(b, a, s, r), HALF, HALF, bufs(1), send_sems, recv_sems, 179
    )
    blocks = [rows_y.dest(j) for j in range(N)]
    feed(0, blocks[0])
    feed(1, blocks[1])
    pl.semaphore_wait(free_sem, 4)
    joined(0, blocks[0])
    for j in range(N):
        rows_x.far(j)
    rows_y.far(0)
    feed(2, blocks[2])
    joined(1, blocks[1])
    rows_y.far(1)
    rows_y.up(0)
    rows_y.down(0)
    feed(3, blocks[3])
    joined(2, blocks[2])
    rows_y.far(2)
    rows_y.up(1)
    rows_y.down(1)
    for j in range(2):
        rows_x.up(j)
        rows_x.down(j)
    joined(3, blocks[3])
    rows_y.far(3)
    for j in range(2, N):
        rows_x.up(j)
        rows_x.down(j)
        rows_y.up(j)
        rows_y.down(j)
    for j in range(N):
        for r in (rows_x, rows_y):
            r.own(j)
            if j == 0:
                r.second_far()
            if j == 1:
                r.second_up()
            if j == 2:
                r.second_down()
    mixed[:HALF, :] = (stream[:HALF, :] + rows_x.total()).astype(jnp.bfloat16)
    mixed[HALF:, :] = (stream[HALF:, :] + rows_y.total()).astype(jnp.bfloat16)
    for done in (ups, downs, rows_x, rows_y):
        done.finish()
    for copy in (*handed, *square_copies):
        copy.wait_send()


def body(
    queries, keys, values, documents, query_gain, key_gain, residual, out_weight, norm_gain, up_weight, down_weight
):
    bf, f32 = jnp.bfloat16, jnp.float32
    cosine, sine = tables(lax.axis_index(("z", "x")))
    return pl.pallas_call(
        layer_kernel,
        out_shape=jax.ShapeDtypeStruct((TOK, TOK), bf),
        in_specs=[ANY] * 13,
        out_specs=VMEM,
        scratch_shapes=[
            pltpu.VMEM((N, 8, TOK, TOK), bf),
            pltpu.VMEM((N, N, 256, TOK), bf),
            pltpu.VMEM((N, N, TOK, 256), bf),
            pltpu.VMEM((2, N, N, TOK, TOK), bf),
            pltpu.VMEM((N, N, TOK, TOK), bf),
            pltpu.VMEM((TOK, TOK), f32),
            pltpu.VMEM((N * HALF, TOK), f32),
            pltpu.VMEM((N, TOK, TOK), bf),
            pltpu.VMEM((8, 8, TOK), f32),
            pltpu.VMEM((TOK, TOK), f32),
            pltpu.VMEM((16, 1, TOK), jnp.int32),
            pltpu.VMEM((TOK, HD), jnp.int32),
            pltpu.VMEM((1, HD), f32),
            pltpu.VMEM((1, HD), f32),
            pltpu.VMEM((8, 1, TOK), f32),
            pltpu.SemaphoreType.DMA((199,)),
            pltpu.SemaphoreType.DMA((199,)),
            pltpu.SemaphoreType.DMA((13,)),
            pltpu.SemaphoreType.REGULAR,
        ],
        compiler_params=pltpu.CompilerParams(
            collective_id=0, has_side_effects=True, vmem_limit_bytes=67043328
        ),
        name="layer",
    )(
        queries, keys, values, documents.reshape(1, TOK), query_gain.reshape(1, HD), key_gain.reshape(1, HD),
        cosine, sine, out_weight, residual, norm_gain.reshape(8, 1, TOK), up_weight, down_weight,
    )


def solution(mesh):
    split = Mesh(mesh.devices.reshape(N, N, N, 2), ("z", "x", "y", "c"))
    sp, tp = ("z", "x"), ("y", "c")
    return jax.shard_map(
        body,
        mesh=split,
        in_specs=(
            P(sp, tp), P(sp, tp), P(sp, tp), P(sp), P(), P(), P(sp, tp), P(tp, None), P(), P(sp, tp), P(tp, sp),
        ),
        out_specs=P(sp, tp),
        check_vma=False,
    )
```

```python
import functools
import jax
import jax.numpy as jnp
from jax import lax
from jax.experimental import pallas as pl
from jax.experimental.pallas import tpu as pltpu
from jax.sharding import Mesh
from jax.sharding import PartitionSpec as P

D = 4096
FF = 16384
HQ = 16
KV = 8
HD = 128
GRID_W = 64
TOK = 512
HALF = 256
N = 4

norm_eps = 1e-06
rope_base = 10000.0
masked_score = -1e30
query_mark = 128.0
key_mark = 96.0

MESH = pl.DeviceIdType.MESH
VMEM = pl.BlockSpec(memory_space=pltpu.VMEM)
ANY = pl.BlockSpec(memory_space=pl.ANY)


def shifted(index, by):
    return lax.rem(index + by + N, N)


def send(src, dst, send_sem, recv_sem, device):
    copy = pltpu.make_async_remote_copy(
        src_ref=src,
        dst_ref=dst,
        send_sem=send_sem,
        recv_sem=recv_sem,
        device_id=device,
        device_id_type=MESH,
    )
    copy.start()
    return copy


def arrived(dst, send_sem, recv_sem, device):
    pltpu.make_async_remote_copy(
        src_ref=dst,
        dst_ref=dst,
        send_sem=send_sem,
        recv_sem=recv_sem,
        device_id=device,
        device_id_type=MESH,
    ).wait_recv()


class TorusGather:
    SENDS = 20

    def __init__(self, first, second, piece, start, rows, send_sems, recv_sems, base):
        self.first, self.second = first, second
        self.a, self.b = lax.axis_index(first), lax.axis_index(second)
        self.piece, self.start, self.rows = piece, start, rows
        self.send_sems, self.recv_sems, self.base = send_sems, recv_sems, base
        self.sent = []

    def order(self, j):
        return (self.a, shifted(self.a, -1), shifted(self.a, 1), shifted(self.a, 2))[j]

    def ref(self, a, b, part):
        rows = self.rows // 2
        if part is None:
            return self.piece(a, b, self.start, self.rows)
        return self.piece(a, b, self.start + part * rows, rows)

    def put(self, k, axis, by, a, b, part):
        here = self.ref(a, b, part)
        device = {axis: shifted(lax.axis_index(axis), by)}
        k += self.base
        self.sent.append(send(here, here, self.send_sems.at[k], self.recv_sems.at[k], device))

    def take(self, k, a, b, part):
        k += self.base
        arrived(self.ref(a, b, part), self.send_sems.at[k], self.recv_sems.at[k], {self.first: self.a})

    def spread(self, j):
        self.put(4 + 4 * j, self.second, 1, self.order(j), self.b, None)
        self.put(5 + 4 * j, self.second, -1, self.order(j), self.b, None)

    def begin(self):
        self.put(0, self.first, 1, self.a, self.b, None)
        self.put(1, self.first, -1, self.a, self.b, None)

    def follow(self):
        for copy in self.sent:
            copy.wait_send()
        self.sent.clear()
        self.spread(0)

    def near(self):
        self.take(0, self.order(1), self.b, None)
        self.put(2, self.first, 1, self.order(1), self.b, 0)
        self.spread(1)
        self.take(1, self.order(2), self.b, None)
        self.put(3, self.first, -1, self.order(2), self.b, 1)
        self.spread(2)

    def far(self):
        self.take(2, self.order(3), self.b, 0)
        self.take(3, self.order(3), self.b, 1)
        self.spread(3)

    def pass_on(self, j):
        low, high = shifted(self.b, -1), shifted(self.b, 1)
        self.take(4 + 4 * j, self.order(j), low, None)
        self.put(6 + 4 * j, self.second, 1, self.order(j), low, 0)
        self.take(5 + 4 * j, self.order(j), high, None)
        self.put(7 + 4 * j, self.second, -1, self.order(j), high, 1)

    def last(self, j):
        self.take(6 + 4 * j, self.order(j), shifted(self.b, 2), 0)
        self.take(7 + 4 * j, self.order(j), shifted(self.b, 2), 1)

    def finish(self):
        for copy in self.sent:
            copy.wait_send()


class Exchange:
    SENDS = 6

    def __init__(self, axis, source, target, stage, rows, send_sems, recv_sems, base, beyond=None):
        self.axis, self.me = axis, lax.axis_index(axis)
        self.source, self.target, self.stage, self.rows = source, target, stage, rows
        self.send_sems, self.recv_sems, self.base = send_sems, recv_sems, base
        self.beyond = beyond or {}
        self.sent = []

    def put(self, k, src, dst, by, beyond=True):
        device = {self.axis: shifted(self.me, by)}
        if beyond:
            device.update(self.beyond)
        k += self.base
        self.sent.append(send(src, dst, self.send_sems.at[k], self.recv_sems.at[k], device))

    def take(self, k, dst):
        k += self.base
        arrived(dst, self.send_sems.at[k], self.recv_sems.at[k], {self.axis: self.me})

    def begin(self):
        half = self.rows // 2
        far = shifted(self.me, 2)
        self.put(2, self.source(far, 0, half), self.stage(0), 1, False)
        self.put(3, self.source(far, half, half), self.stage(1), -1, False)
        self.put(0, self.source(shifted(self.me, 1), 0, self.rows), self.target(self.me, 0, self.rows), 1)
        self.put(1, self.source(shifted(self.me, -1), 0, self.rows), self.target(self.me, 0, self.rows), -1)

    def pass_on(self):
        half = self.rows // 2
        self.take(2, self.stage(0))
        self.put(4, self.stage(0), self.target(shifted(self.me, -1), 0, half), 1)
        self.take(3, self.stage(1))
        self.put(5, self.stage(1), self.target(shifted(self.me, 1), half, half), -1)

    def last(self):
        half = self.rows // 2
        self.take(0, self.target(shifted(self.me, -1), 0, self.rows))
        self.take(1, self.target(shifted(self.me, 1), 0, self.rows))
        self.take(4, self.target(shifted(self.me, 2), 0, half))
        self.take(5, self.target(shifted(self.me, 2), half, half))

    def finish(self):
        for copy in self.sent:
            copy.wait_send()


def swapped(u):
    lane = lax.broadcasted_iota(jnp.int32, u.shape, 1)
    ahead = pltpu.roll(u, HD - HD // 4, 1)
    behind = pltpu.roll(u, HD // 4, 1)
    return jnp.where(lax.rem(lane, HD // 2) < HD // 4, ahead, behind)


def rotated(u, gain, cosine, sine):
    u = u.astype(jnp.float32)
    u = u * lax.rsqrt(jnp.mean(u * u, axis=-1, keepdims=True) + norm_eps) * gain
    return (u * cosine + swapped(u) * sine).astype(jnp.bfloat16)


def barrier_with(peers):
    barrier = pltpu.get_barrier_semaphore()
    for peer in peers:
        pl.semaphore_signal(barrier, inc=1, device_id=peer, device_id_type=MESH)
    return lambda: pl.semaphore_wait(barrier, len(peers))


def tables(sp):
    position = sp * TOK + jnp.arange(TOK, dtype=jnp.int32)
    lane = jnp.arange(HD, dtype=jnp.int32)
    quarter = HD // 4
    inverse_freq = rope_base ** (-(lane % quarter).astype(jnp.float32) / quarter)
    place = jnp.where(
        lane[None, :] < HD // 2, (position // GRID_W)[:, None], (position % GRID_W)[:, None]
    ).astype(jnp.float32)
    angles = place * inverse_freq[None, :]
    sign = jnp.where(lane % (HD // 2) < quarter, -1.0, 1.0)
    return jnp.cos(angles), jnp.sin(angles) * sign[None, :]


class RingGather:
    SENDS = 4

    def __init__(self, axis, piece, own, send_sems, recv_sems, base):
        self.axis, self.me = axis, lax.axis_index(axis)
        self.piece, self.own = piece, own
        self.send_sems, self.recv_sems, self.base = send_sems, recv_sems, base
        self.sent = []

    def put(self, k, src, dst, by):
        device = {self.axis: shifted(self.me, by)}
        k += self.base
        self.sent.append(send(src, dst, self.send_sems.at[k], self.recv_sems.at[k], device))

    def take(self, k, dst):
        k += self.base
        arrived(dst, self.send_sems.at[k], self.recv_sems.at[k], {self.axis: self.me})

    def begin(self):
        self.put(0, self.own, self.piece(self.me, None), 1)
        self.put(1, self.own, self.piece(self.me, None), -1)

    def low(self):
        who = shifted(self.me, -1)
        self.take(0, self.piece(who, None))
        self.put(2, self.piece(who, 0), self.piece(who, 0), 1)

    def high(self):
        who = shifted(self.me, 1)
        self.take(1, self.piece(who, None))
        self.put(3, self.piece(who, 1), self.piece(who, 1), -1)

    def far(self):
        who = shifted(self.me, 2)
        self.take(2, self.piece(who, 0))
        self.take(3, self.piece(who, 1))

    def finish(self):
        for copy in self.sent:
            copy.wait_send()


class TorusReduce:
    SENDS = 20

    def __init__(self, first, second, piece, start, rows, bufs, send_sems, recv_sems, base):
        self.first, self.second = first, second
        self.a, self.b = lax.axis_index(first), lax.axis_index(second)
        self.piece, self.start, self.rows = piece, start, rows
        self.buf = bufs
        self.send_sems, self.recv_sems, self.base = send_sems, recv_sems, base
        self.sent = []

    def dest(self, j):
        return shifted(self.b, (2, 1, -1, 0)[j])

    def ref(self, a, b, part):
        rows = self.rows // 2
        if part is None:
            return self.piece(a, b, self.start, self.rows)
        return self.piece(a, b, self.start + part * rows, rows)

    def put(self, k, axis, by, src, dst):
        device = {axis: shifted(lax.axis_index(axis), by)}
        k += self.base
        self.sent.append(send(src, dst, self.send_sems.at[k], self.recv_sems.at[k], device))

    def take(self, k, dst):
        k += self.base
        arrived(dst, self.send_sems.at[k], self.recv_sems.at[k], {self.first: self.a})

    @staticmethod
    def add(into, *others):
        total = into[...].astype(jnp.float32)
        for other in others:
            total = total + other[...].astype(jnp.float32)
        into[...] = total.astype(into.dtype)

    def far(self, j):
        a, b = shifted(self.a, 2), self.dest(j)
        self.put(4 * j, self.first, 1, self.ref(a, b, 0), self.buf("far_first", 0, j))
        self.put(4 * j + 1, self.first, -1, self.ref(a, b, 1), self.buf("far_first", 1, j))

    def up(self, j):
        a, b = shifted(self.a, 1), self.dest(j)
        self.take(4 * j, self.buf("far_first", 0, j))
        self.add(self.ref(a, b, 0), self.buf("far_first", 0, j))
        self.put(4 * j + 2, self.first, 1, self.ref(a, b, None), self.buf("near_first", 0, j))

    def down(self, j):
        a, b = shifted(self.a, -1), self.dest(j)
        self.take(4 * j + 1, self.buf("far_first", 1, j))
        self.add(self.ref(a, b, 1), self.buf("far_first", 1, j))
        self.put(4 * j + 3, self.first, -1, self.ref(a, b, None), self.buf("near_first", 1, j))

    def own(self, j):
        self.take(4 * j + 2, self.buf("near_first", 0, j))
        self.take(4 * j + 3, self.buf("near_first", 1, j))
        self.add(self.ref(self.a, self.dest(j), None), self.buf("near_first", 0, j), self.buf("near_first", 1, j))

    def second_far(self):
        b = shifted(self.b, 2)
        self.put(16, self.second, 1, self.ref(self.a, b, 0), self.buf("far_second", 0, 0))
        self.put(17, self.second, -1, self.ref(self.a, b, 1), self.buf("far_second", 1, 0))

    def second_up(self):
        b = shifted(self.b, 1)
        self.take(16, self.buf("far_second", 0, 0))
        self.add(self.ref(self.a, b, 0), self.buf("far_second", 0, 0))
        self.put(18, self.second, 1, self.ref(self.a, b, None), self.buf("near_second", 0, 0))

    def second_down(self):
        b = shifted(self.b, -1)
        self.take(17, self.buf("far_second", 1, 0))
        self.add(self.ref(self.a, b, 1), self.buf("far_second", 1, 0))
        self.put(19, self.second, -1, self.ref(self.a, b, None), self.buf("near_second", 1, 0))

    def total(self):
        self.take(18, self.buf("near_second", 0, 0))
        self.take(19, self.buf("near_second", 1, 0))
        total = self.ref(self.a, self.b, None)[...].astype(jnp.float32)
        total = total + self.buf("near_second", 0, 0)[...].astype(jnp.float32)
        return total + self.buf("near_second", 1, 0)[...].astype(jnp.float32)

    def finish(self):
        for copy in self.sent:
            copy.wait_send()


def layer_kernel(
    queries, keys, values, documents, query_gain, key_gain, cosines, sines,
    out_w, residuals, norm_gains, up_w, down_w, mixed,
    x_all, up_all, down_all, sums, theirs, stream, hidden, squared, squares,
    hidden_early, docs, doc_column, q_gain, k_gain, gains, send_sems, recv_sems, local_sems, free_sem,
):
    z, x, y, c = (lax.axis_index(n) for n in ("z", "x", "y", "c"))
    other = 1 - c
    sp = z * N + x
    tp = y * 2 + c
    plane = [
        {"z": shifted(z, dz), "x": shifted(x, dx)} for dz in range(N) for dx in range(N) if dz or dx
    ]
    group = [{"y": shifted(y, dy), "c": cc} for dy in range(N) for cc in (c, other) if dy or cc is other]
    wait = barrier_with(plane + group)

    def kv_place(zz, xx, start, rows):
        return sums.at[1, zz, xx, pl.ds(start, rows), :]

    def att_slot(t, part):
        rows = pl.ds(0, TOK) if part is None else pl.ds(part * HALF, HALF)
        return sums.at[0, lax.div(t, 4), lax.rem(t, 4), rows, pl.ds(0, 256)]

    def col_slot(t, start=0, rows=256):
        return theirs.at[lax.div(t, 4), lax.rem(t, 4), pl.ds(start, rows), :]

    def thousand(index):
        return pl.ds(pl.multiple_of(index * TOK, TOK), TOK)

    q_in = theirs.at[2, 0, :, pl.ds(0, 2 * HD)]
    k_in = theirs.at[2, 1, :, pl.ds(0, HD)]
    v_in = theirs.at[2, 2, :, pl.ds(0, HD)]
    q_rot = theirs.at[2, 3]
    residual = theirs.at[3, 0]
    cosine = stream.at[:, pl.ds(2 * HD, HD)]
    sine = stream.at[:, pl.ds(3 * HD, HD)]

    def local(i, src, dst):
        copy = pltpu.make_async_copy(src, dst, local_sems.at[i])
        copy.start()
        return copy

    first = [
        local(0, keys, k_in),
        local(1, values, v_in),
        local(2, cosines, cosine),
        local(3, sines, sine),
        local(4, key_gain, k_gain),
        local(5, documents, docs.at[sp]),
    ]
    second = [local(6, queries, q_in), local(7, query_gain, q_gain)]
    third = [
        local(8, residuals, residual),
        local(9, norm_gains, gains),
        local(10, out_w.at[:, thousand(tp)], col_slot(tp)),
    ]
    fourth = [
        local(11, up_w.at[:, thousand(x)], up_all.at[z, x]),
        local(12, down_w.at[thousand(x), :], down_all.at[z, x]),
    ]
    for copy in first:
        copy.wait()
    mine = kv_place(z, x, 0, 2 * HD)
    turned = jnp.transpose(rotated(k_in[...], k_gain[...], cosine[...], sine[...]).astype(jnp.float32))
    mine[HD:, :] = turned.astype(jnp.bfloat16)
    for i in range(TOK // HD):
        mine[:HD, i * HD : (i + 1) * HD] = v_in[i * HD : (i + 1) * HD, :]

    def mark(zz, xx):
        row = lax.broadcasted_iota(jnp.int32, (HD, TOK), 0)
        hot = jnp.where(row == docs[zz * N + xx], key_mark, 0.0)
        sums[1, zz, xx, 2 * HD : 3 * HD, :] = hot.astype(jnp.bfloat16)

    mark(z, x)
    column = jnp.broadcast_to(docs[sp].astype(jnp.float32), (HD, TOK))
    doc_column[...] = jnp.transpose(column).astype(jnp.int32)
    wait()

    kvs = TorusGather("x", "z", lambda a, b, s, r: kv_place(b, a, s, r), 0, 2 * HD, send_sems, recv_sems, 0)
    ups_across = Exchange(
        "x",
        lambda to, s, r: up_w.at[pl.ds(s, r), thousand(to)],
        lambda who, s, r: up_all.at[z, who, pl.ds(s, r), :],
        lambda i: squared.at[0, pl.ds(128 * i, 128), :],
        256, send_sems, recv_sems, 20,
    )
    downs_across = Exchange(
        "x",
        lambda to, s, r: down_w.at[pl.ds(pl.multiple_of(to * TOK + s, HALF), r), :],
        lambda who, s, r: down_all.at[z, who, pl.ds(s, r), :],
        lambda i: squared.at[1, pl.ds(256 * i, 256), pl.ds(0, 256)],
        512, send_sems, recv_sems, 26,
    )
    columns = []
    for i, cc in enumerate((c, other)):
        ex = Exchange(
            "y",
            lambda to, s, r, cc=cc: out_w.at[pl.ds(s, r), thousand(to * 2 + cc)],
            lambda who, s, r: col_slot(who * 2 + c, s, r),
            lambda k, i=i: squared.at[2, pl.ds(128 * (2 * i + k), 128), :],
            256, send_sems, recv_sems, 32 + 6 * i, {"c": cc},
        )
        ex.landed = lambda who, s, r, cc=cc: col_slot(who * 2 + cc, s, r)
        columns.append(ex)
    kvs.begin()
    kvs.spread(0)
    doc_copies = [
        send(docs.at[sp], docs.at[sp], send_sems.at[45 + i], recv_sems.at[45 + i], peer)
        for i, peer in enumerate(plane)
    ]
    for ex in columns:
        ex.begin()
    twin = send(
        out_w.at[:, thousand(y * 2 + other)], col_slot(tp), send_sems.at[44], recv_sems.at[44], {"c": other}
    )

    for copy in second:
        copy.wait()
    lane = lax.broadcasted_iota(jnp.int32, (TOK, HD), 1)
    hot = jnp.where(lane == doc_column[...], query_mark, 0.0).astype(jnp.bfloat16)
    for h in range(2):
        turn = rotated(q_in[:, h * HD : (h + 1) * HD], q_gain[...], cosine[...], sine[...])
        for t in range(2):
            rows, part = slice(h * HALF, (h + 1) * HALF), slice(t * HALF, (t + 1) * HALF)
            q_rot[rows, 2 * t * HD : (2 * t + 1) * HD] = turn[part]
            q_rot[rows, (2 * t + 1) * HD : (2 * t + 2) * HD] = hot[part]
    hidden[:, :HD] = jnp.zeros((2 * TOK, HD), jnp.float32)
    hidden[:, HD : 2 * HD] = jnp.full((2 * TOK, HD), masked_score, jnp.float32)
    hidden[:, 2 * HD : 3 * HD] = jnp.zeros((2 * TOK, HD), jnp.float32)
    scale = HD ** (-0.5) * 1.4426950408889634

    def attend(count, which):
        @pl.loop(0, 2)
        def _(t):
            rows = pl.ds(pl.multiple_of(t * TOK, TOK), TOK)
            q = q_rot[:, pl.ds(pl.multiple_of(t * HALF, HALF), HALF)]
            cuts = [slice(i * HD, (i + 1) * HD) for i in range(4)]

            def step(i, carry):
                top, total, weighted = carry
                zz, xx = which(i)
                packed = sums[1, zz, xx, :HD, :]
                v = jnp.concatenate([packed[:, cut] for cut in cuts], axis=0)
                s = jnp.dot(q, sums[1, zz, xx, HD : 3 * HD, :], preferred_element_type=jnp.float32)
                s = [s[:, cut] for cut in cuts]
                most = jnp.maximum(jnp.maximum(s[0], s[1]), jnp.maximum(s[2], s[3]))
                new_top = jnp.maximum(top, jnp.max(most, axis=-1, keepdims=True))
                p = [jnp.exp2((part - new_top) * scale) for part in s]
                fade = jnp.exp2((top - new_top) * scale)
                total = total * fade + ((p[0] + p[1]) + (p[2] + p[3]))
                low = jnp.concatenate([part.astype(jnp.bfloat16) for part in p], axis=1)
                weighted = weighted * fade + jnp.dot(low, v, preferred_element_type=jnp.float32)
                return new_top, total, weighted

            start = (hidden[rows, cuts[1]], hidden[rows, cuts[2]], hidden[rows, cuts[0]])
            top, total, weighted = lax.fori_loop(0, count, step, start)
            hidden[rows, cuts[1]] = top
            hidden[rows, cuts[2]] = total
            hidden[rows, cuts[0]] = weighted

    attend(1, lambda i: (z, x))
    kvs.near()
    kvs.far()
    ups_across.begin()
    downs_across.begin()
    for i, peer in enumerate(plane):
        dz, dx = divmod(i + 1, N)
        arrived(
            docs.at[shifted(z, -dz) * N + shifted(x, -dx)], send_sems.at[45 + i], recv_sems.at[45 + i], {"z": z}
        )

    @pl.loop(1, 16)
    def _(i):
        mark(lax.rem(z + lax.div(i, N), N), lax.rem(x + i, N))

    attend(3, lambda i: (z, lax.rem(x + 1 + i, N)))
    kvs.pass_on(0)
    kvs.pass_on(1)
    for ex in columns:
        ex.pass_on()
    attend(4, lambda i: (lax.rem(z + 1 + 2 * lax.rem(i, 2), N), lax.rem(x + N - lax.div(i, 2), N)))
    kvs.pass_on(2)
    kvs.pass_on(3)
    ups_across.pass_on()
    downs_across.pass_on()
    attend(4, lambda i: (lax.rem(z + 1 + 2 * lax.rem(i, 2), N), lax.rem(x + 1 + lax.div(i, 2), N)))
    kvs.last(0)
    kvs.last(1)
    attend(2, lambda i: (lax.rem(z + 2, N), lax.rem(x + N - i, N)))
    kvs.last(2)
    kvs.last(3)
    def half_of(ref, z_at, part):
        at = ref.at[z_at]
        return at if part is None else at.at[pl.ds(2 * part, 2)]

    ups = RingGather(
        "z", lambda who, part: half_of(up_all, who, part), up_all.at[z], send_sems, recv_sems, 68
    )
    downs = RingGather(
        "z", lambda who, part: half_of(down_all, who, part), down_all.at[z], send_sems, recv_sems, 72
    )
    for copy in fourth:
        copy.wait()
    ups_across.last()
    ups.begin()
    attend(2, lambda i: (lax.rem(z + 2, N), lax.rem(x + 1 + i, N)))

    att = att_slot(tp, None)
    for t in range(2):
        for h in range(2):
            rows = slice(t * TOK + h * HALF, t * TOK + (h + 1) * HALF)
            total = jnp.sum(hidden[rows, 2 * HD : 3 * HD], axis=-1, keepdims=True)
            att[t * HALF : (t + 1) * HALF, h * HD : (h + 1) * HD] = (hidden[rows, :HD] / total).astype(jnp.bfloat16)

    handed = []

    def hand(k, src, dst):
        handed.append(send(src, dst, send_sems.at[k], recv_sems.at[k], {"c": other}))

    def taken(k, dst):
        arrived(dst, send_sems.at[k], recv_sems.at[k], {"c": c})

    heads = RingGather("y", lambda who, part: att_slot(who * 2 + c, part), att, send_sems, recv_sems, 60)
    heads.begin()
    hand(64, att, att)

    for copy in third:
        copy.wait()
    for ex in columns:
        ex.target = ex.landed
        ex.last()
    arrived(col_slot(y * 2 + other), send_sems.at[44], recv_sems.at[44], {"c": c})

    def project(t):
        part = jnp.dot(att_slot(t, None)[...], col_slot(t)[...], preferred_element_type=jnp.float32)
        stream[...] += part.astype(jnp.bfloat16).astype(jnp.float32)

    y_low, y_high, y_far = shifted(y, -1), shifted(y, 1), shifted(y, 2)
    stream[...] = residual[...].astype(jnp.float32)
    project(tp)
    heads.low()
    hand(65, att_slot(y_low * 2 + c, None), att_slot(y_low * 2 + c, None))
    heads.high()
    hand(66, att_slot(y_high * 2 + c, None), att_slot(y_high * 2 + c, None))
    taken(64, att_slot(y * 2 + other, None))
    project(y * 2 + other)
    project(y_low * 2 + c)
    project(y_high * 2 + c)
    downs_across.last()
    heads.far()
    hand(67, att_slot(y_far * 2 + c, None), att_slot(y_far * 2 + c, None))
    taken(65, att_slot(y_low * 2 + other, None))
    project(y_low * 2 + other)
    taken(66, att_slot(y_high * 2 + other, None))
    project(y_high * 2 + other)
    project(y_far * 2 + c)
    taken(67, att_slot(y_far * 2 + other, None))
    project(y_far * 2 + other)

    whole = stream[...]
    partial = jnp.sum(whole * whole, axis=-1, keepdims=True)
    squares[tp] = jnp.transpose(jnp.broadcast_to(partial, (TOK, HD)))[:8]
    square_copies = [
        send(squares.at[tp], squares.at[tp], send_sems.at[76 + i], recv_sems.at[76 + i], peer)
        for i, peer in enumerate(group)
    ]
    for done in (heads, kvs, ups_across, downs_across, *columns):
        done.finish()
    for copy in (*handed, *doc_copies, twin):
        copy.wait_send()
    handed.clear()
    i = 0
    for dy in range(N):
        for cc in (c, other):
            if dy or cc is other:
                arrived(squares.at[shifted(y, -dy) * 2 + cc], send_sems.at[76 + i], recv_sems.at[76 + i], {"c": c})
                i += 1
    full = squares[0]
    for t in range(1, 8):
        full = full + squares[t]
    full = jnp.transpose(jnp.broadcast_to(full[:1], (HD, TOK)))
    inverse = lax.rsqrt(full[:, :1] / D + norm_eps)
    x_all[x, tp] = (stream[...] * inverse * gains[tp]).astype(jnp.bfloat16)

    def place(xx, yy, start, rows):
        return x_all.at[xx, yy * 2 + c, pl.ds(start, rows), :]

    gathers = [
        TorusGather("y", "x", lambda a, b, s, r: place(b, a, s, r), 0, HALF, send_sems, recv_sems, 83),
        TorusGather("x", "y", place, HALF, HALF, send_sems, recv_sems, 103),
    ]

    def share(n, j, i):
        g = gathers[n]
        ref = g.ref(g.order(j), shifted(g.b, (0, -1, 1, 2)[i]), None)
        hand(123 + 16 * n + 4 * j + i, ref, ref)

    def shared(n, j, i):
        g = gathers[n]
        a, b = g.order(j), shifted(g.b, (0, -1, 1, 2)[i])
        xx, yy = (b, a) if n == 0 else (a, b)
        taken(123 + 16 * n + 4 * j + i, x_all.at[xx, yy * 2 + other, pl.ds(n * HALF, HALF), :])

    def weight(t):
        return up_all[lax.div(t, 2), pl.ds(2 * lax.rem(t, 2), 2)].reshape(TOK, TOK)

    def square(value):
        positive = jnp.maximum(value, 0.0)
        return (positive * positive).astype(jnp.bfloat16)

    def early(blocks, first, count, step, clear, store):
        rows = HALF * len(blocks)
        acc = hidden_early.at[pl.ds(0, rows)]
        if clear:
            acc[...] = jnp.zeros_like(acc)

        @pl.loop(0, count)
        def _(i):
            t = lax.rem(first + step * i, 8)
            parts = [x_all[xx, t, :HALF, :] for xx in blocks]
            part = parts[0] if len(parts) == 1 else jnp.concatenate(parts, axis=0)
            acc[...] += jnp.dot(part, weight(t), preferred_element_type=jnp.float32)

        if store:
            for i, xx in enumerate(blocks):
                squared[xx, :HALF, :] = square(hidden_early[i * HALF : (i + 1) * HALF, :])

    def late(first, count, step):
        @pl.loop(0, count)
        def _(i):
            t = lax.rem(first + step * i, 8)
            rows = x_all[:, t, HALF:, :].reshape(N * HALF, TOK)
            hidden[...] += jnp.dot(rows, weight(t), preferred_element_type=jnp.float32)

    for g in gathers:
        g.begin()
    for n in range(2):
        share(n, 0, 0)
    ups.low()
    ups.high()
    downs.begin()
    for g in gathers:
        g.follow()
    hidden[...] = jnp.zeros_like(hidden)
    for n, g in enumerate(gathers):
        g.near()
        share(n, 1, 0)
        share(n, 2, 0)
    for n, g in enumerate(gathers):
        g.far()
        share(n, 3, 0)
    ups.far()
    for n in range(2):
        for j in range(N):
            shared(n, j, 0)
        if n == 0:
            early([x], 0, 8, 1, True, True)
    for j in range(N):
        for n, g in enumerate(gathers):
            g.pass_on(j)
            share(n, j, 1)
            share(n, j, 2)
    late(2 * (y + 3) + c, 3, 2)
    late(2 * y + other, 1, 2)
    for j in range(N):
        for i in (1, 2):
            for n in range(2):
                shared(n, j, i)
    late(2 * (y + 3) + other, 2, 4)
    downs.low()
    downs.high()
    sides = [shifted(x, -1), shifted(x, 1)]
    early(sides, 0, 4, 1, True, False)
    for j in range(N):
        for n, g in enumerate(gathers):
            g.last(j)
            share(n, j, 3)
    early(sides, 4, 4, 1, False, True)
    opposite = [shifted(x, 2)]
    late(2 * (y + 2) + c, 1, 2)
    early(opposite, c, 4, 2, True, False)
    for n in range(2):
        for j in range(N):
            shared(n, j, 3)
    early(opposite, other, 4, 2, False, True)
    late(2 * (y + 2) + other, 1, 2)
    @pl.loop(0, N)
    def _(xx):
        rows = pl.ds(pl.multiple_of(xx * HALF, HALF), HALF)
        squared[xx, HALF:, :] = square(hidden[rows, :])

    for g in gathers:
        g.finish()
    for copy in handed:
        copy.wait_send()
    handed.clear()
    for peer in ({"x": shifted(x, 1)}, {"x": shifted(x, -1)}, {"y": shifted(y, 1)}, {"y": shifted(y, -1)}):
        pl.semaphore_signal(free_sem, inc=1, device_id=peer, device_id_type=MESH)

    def column(cc, xx, yy):
        pair = [down_all[yy, 2 * cc + part] for part in range(2)]
        sums[cc, xx, yy] = jnp.dot(
            squared[xx], jnp.concatenate(pair, axis=1), preferred_element_type=jnp.float32
        ).astype(jnp.bfloat16)

    def near_columns(cc, xx):
        @pl.loop(0, N - 1)
        def _(i):
            column(cc, xx, lax.rem(z + 3 + i, N))

    def far_column(cc, xx):
        column(cc, xx, shifted(z, 2))

    def hand_on(i, xx, offsets):
        for k in offsets:
            yy = shifted(z, k)
            hand((155, 199, 203, 207)[i] + k % N, sums.at[other, xx, yy], theirs.at[xx, yy])

    def joined(i, xx):
        for k in range(N):
            taken((155, 199, 203, 207)[i] + k, theirs.at[xx, shifted(z, k)])

        @pl.loop(0, N)
        def _(yy):
            TorusReduce.add(sums.at[c, xx, yy], theirs.at[xx, yy])

    def sum_place(xx, yy, start, rows):
        return sums.at[c, xx, yy, pl.ds(start, rows), :]

    def bufs(n):
        def buf(kind, way, j):
            if kind == "near_first":
                return x_all.at[n, 4 * way + j, pl.ds(0, HALF), :]
            if kind == "far_first":
                return x_all.at[n, 4 * way + j, pl.ds(HALF, HALF // 2), :]
            if kind == "near_second":
                return x_all.at[2, 2 * n + way, pl.ds(0, HALF), :]
            return x_all.at[2, 2 * n + way, pl.ds(HALF, HALF // 2), :]

        return buf

    rows_x = TorusReduce("x", "y", sum_place, 0, HALF, bufs(0), send_sems, recv_sems, 159)
    rows_y = TorusReduce(
        "y", "x", lambda a, b, s, r: sum_place(b, a, s, r), HALF, HALF, bufs(1), send_sems, recv_sems, 179
    )
    blocks = [rows_y.dest(j) for j in range(N)]
    for i in range(2):
        near_columns(other, blocks[i])
        hand_on(i, blocks[i], (-1, 0, 1))
    near_columns(c, blocks[0])
    downs.far()
    far_column(other, blocks[0])
    hand_on(0, blocks[0], (2,))
    far_column(c, blocks[0])
    far_column(other, blocks[1])
    hand_on(1, blocks[1], (2,))
    pl.semaphore_wait(free_sem, 4)
    joined(0, blocks[0])
    for j in range(N):
        rows_x.far(j)
    rows_y.far(0)
    near_columns(c, blocks[1])
    far_column(c, blocks[1])
    joined(1, blocks[1])
    rows_y.far(1)
    near_columns(other, blocks[2])
    far_column(other, blocks[2])
    hand_on(2, blocks[2], (-1, 0, 1, 2))
    rows_y.up(0)
    rows_y.down(0)
    near_columns(c, blocks[2])
    far_column(c, blocks[2])
    near_columns(other, blocks[3])
    far_column(other, blocks[3])
    hand_on(3, blocks[3], (-1, 0, 1, 2))
    joined(2, blocks[2])
    rows_y.far(2)
    rows_y.up(1)
    rows_y.down(1)
    near_columns(c, blocks[3])
    far_column(c, blocks[3])
    joined(3, blocks[3])
    rows_y.far(3)
    for j in range(2):
        rows_x.up(j)
        rows_x.down(j)
    rows_y.up(2)
    rows_y.down(2)
    rows_y.own(0)
    rows_y.second_far()
    for j in range(2, N):
        rows_x.up(j)
        rows_x.down(j)
    rows_y.up(3)
    rows_y.down(3)
    rows_y.own(1)
    rows_y.second_up()
    rows_x.own(0)
    rows_x.second_far()
    rows_x.own(1)
    rows_y.own(2)
    rows_y.second_down()
    rows_x.second_up()
    rows_x.own(2)
    rows_x.second_down()
    rows_y.own(3)
    rows_x.own(3)
    mixed[:HALF, :] = (stream[:HALF, :] + rows_x.total()).astype(jnp.bfloat16)
    mixed[HALF:, :] = (stream[HALF:, :] + rows_y.total()).astype(jnp.bfloat16)
    for done in (ups, downs, rows_x, rows_y):
        done.finish()
    for copy in (*handed, *square_copies):
        copy.wait_send()


def body(
    queries, keys, values, documents, query_gain, key_gain, residual, out_weight, norm_gain, up_weight, down_weight
):
    bf, f32 = jnp.bfloat16, jnp.float32
    cosine, sine = tables(lax.axis_index(("z", "x")))
    return pl.pallas_call(
        layer_kernel,
        out_shape=jax.ShapeDtypeStruct((TOK, TOK), bf),
        in_specs=[ANY] * 13,
        out_specs=VMEM,
        scratch_shapes=[
            pltpu.VMEM((N, 8, TOK, TOK), bf),
            pltpu.VMEM((N, N, 256, TOK), bf),
            pltpu.VMEM((N, N, TOK, 256), bf),
            pltpu.VMEM((2, N, N, TOK, TOK), bf),
            pltpu.VMEM((N, N, TOK, TOK), bf),
            pltpu.VMEM((TOK, TOK), f32),
            pltpu.VMEM((N * HALF, TOK), f32),
            pltpu.VMEM((N, TOK, TOK), bf),
            pltpu.VMEM((8, 8, TOK), f32),
            pltpu.VMEM((TOK, TOK), f32),
            pltpu.VMEM((16, 1, TOK), jnp.int32),
            pltpu.VMEM((TOK, HD), jnp.int32),
            pltpu.VMEM((1, HD), f32),
            pltpu.VMEM((1, HD), f32),
            pltpu.VMEM((8, 1, TOK), f32),
            pltpu.SemaphoreType.DMA((211,)),
            pltpu.SemaphoreType.DMA((211,)),
            pltpu.SemaphoreType.DMA((13,)),
            pltpu.SemaphoreType.REGULAR,
        ],
        compiler_params=pltpu.CompilerParams(
            collective_id=0, has_side_effects=True, vmem_limit_bytes=67043328
        ),
        name="layer",
    )(
        queries, keys, values, documents.reshape(1, TOK), query_gain.reshape(1, HD), key_gain.reshape(1, HD),
        cosine, sine, out_weight, residual, norm_gain.reshape(8, 1, TOK), up_weight, down_weight,
    )


def solution(mesh):
    split = Mesh(mesh.devices.reshape(N, N, N, 2), ("z", "x", "y", "c"))
    sp, tp = ("z", "x"), ("y", "c")
    return jax.shard_map(
        body,
        mesh=split,
        in_specs=(
            P(sp, tp), P(sp, tp), P(sp, tp), P(sp), P(), P(), P(sp, tp), P(tp, None), P(), P(sp, tp), P(tp, sp),
        ),
        out_specs=P(sp, tp),
        check_vma=False,
    )
```

```python
import functools
import jax
import jax.numpy as jnp
import numpy as np
from jax import lax
from jax.experimental import pallas as pl
from jax.experimental.pallas import tpu as pltpu
from jax.sharding import Mesh
from jax.sharding import PartitionSpec as P

D = 4096
FF = 16384
HQ = 16
KV = 8
HD = 128
GRID_W = 64
TOK = 512
HALF = 256
N = 4

norm_eps = 1e-06
rope_base = 10000.0
masked_score = -1e30
query_mark = 128.0
key_mark = 96.0

MESH = pl.DeviceIdType.MESH
VMEM = pl.BlockSpec(memory_space=pltpu.VMEM)
ANY = pl.BlockSpec(memory_space=pl.ANY)


def shifted(index, by):
    return lax.rem(index + by + N, N)


def send(src, dst, send_sem, recv_sem, device):
    copy = pltpu.make_async_remote_copy(
        src_ref=src,
        dst_ref=dst,
        send_sem=send_sem,
        recv_sem=recv_sem,
        device_id=device,
        device_id_type=MESH,
    )
    copy.start()
    return copy


def arrived(dst, send_sem, recv_sem, device):
    pltpu.make_async_remote_copy(
        src_ref=dst,
        dst_ref=dst,
        send_sem=send_sem,
        recv_sem=recv_sem,
        device_id=device,
        device_id_type=MESH,
    ).wait_recv()


class TorusGather:
    SENDS = 20

    def __init__(self, first, second, piece, start, rows, send_sems, recv_sems, base):
        self.first, self.second = first, second
        self.a, self.b = lax.axis_index(first), lax.axis_index(second)
        self.piece, self.start, self.rows = piece, start, rows
        self.send_sems, self.recv_sems, self.base = send_sems, recv_sems, base
        self.sent = []

    def order(self, j):
        return (self.a, shifted(self.a, -1), shifted(self.a, 1), shifted(self.a, 2))[j]

    def ref(self, a, b, part):
        rows = self.rows // 2
        if part is None:
            return self.piece(a, b, self.start, self.rows)
        return self.piece(a, b, self.start + part * rows, rows)

    def put(self, k, axis, by, a, b, part):
        here = self.ref(a, b, part)
        device = {axis: shifted(lax.axis_index(axis), by)}
        k += self.base
        self.sent.append(send(here, here, self.send_sems.at[k], self.recv_sems.at[k], device))

    def take(self, k, a, b, part):
        k += self.base
        arrived(self.ref(a, b, part), self.send_sems.at[k], self.recv_sems.at[k], {self.first: self.a})

    def spread(self, j):
        self.put(4 + 4 * j, self.second, 1, self.order(j), self.b, None)
        self.put(5 + 4 * j, self.second, -1, self.order(j), self.b, None)

    def begin(self):
        self.put(0, self.first, 1, self.a, self.b, None)
        self.put(1, self.first, -1, self.a, self.b, None)

    def follow(self):
        for copy in self.sent:
            copy.wait_send()
        self.sent.clear()
        self.spread(0)

    def near(self):
        self.take(0, self.order(1), self.b, None)
        self.put(2, self.first, 1, self.order(1), self.b, 0)
        self.spread(1)
        self.take(1, self.order(2), self.b, None)
        self.put(3, self.first, -1, self.order(2), self.b, 1)
        self.spread(2)

    def far(self):
        self.take(2, self.order(3), self.b, 0)
        self.take(3, self.order(3), self.b, 1)
        self.spread(3)

    def pass_on(self, j):
        low, high = shifted(self.b, -1), shifted(self.b, 1)
        self.take(4 + 4 * j, self.order(j), low, None)
        self.put(6 + 4 * j, self.second, 1, self.order(j), low, 0)
        self.take(5 + 4 * j, self.order(j), high, None)
        self.put(7 + 4 * j, self.second, -1, self.order(j), high, 1)

    def last(self, j):
        self.take(6 + 4 * j, self.order(j), shifted(self.b, 2), 0)
        self.take(7 + 4 * j, self.order(j), shifted(self.b, 2), 1)

    def finish(self):
        for copy in self.sent:
            copy.wait_send()


class Exchange:
    SENDS = 6

    def __init__(self, axis, source, target, stage, rows, send_sems, recv_sems, base, beyond=None):
        self.axis, self.me = axis, lax.axis_index(axis)
        self.source, self.target, self.stage, self.rows = source, target, stage, rows
        self.send_sems, self.recv_sems, self.base = send_sems, recv_sems, base
        self.beyond = beyond or {}
        self.sent = []

    def put(self, k, src, dst, by, beyond=True):
        device = {self.axis: shifted(self.me, by)}
        if beyond:
            device.update(self.beyond)
        k += self.base
        self.sent.append(send(src, dst, self.send_sems.at[k], self.recv_sems.at[k], device))

    def take(self, k, dst):
        k += self.base
        arrived(dst, self.send_sems.at[k], self.recv_sems.at[k], {self.axis: self.me})

    def begin(self):
        half = self.rows // 2
        far = shifted(self.me, 2)
        self.put(2, self.source(far, 0, half), self.stage(0), 1, False)
        self.put(3, self.source(far, half, half), self.stage(1), -1, False)
        self.put(0, self.source(shifted(self.me, 1), 0, self.rows), self.target(self.me, 0, self.rows), 1)
        self.put(1, self.source(shifted(self.me, -1), 0, self.rows), self.target(self.me, 0, self.rows), -1)

    def pass_on(self):
        half = self.rows // 2
        self.take(2, self.stage(0))
        self.put(4, self.stage(0), self.target(shifted(self.me, -1), 0, half), 1)
        self.take(3, self.stage(1))
        self.put(5, self.stage(1), self.target(shifted(self.me, 1), half, half), -1)

    def last(self):
        half = self.rows // 2
        self.take(0, self.target(shifted(self.me, -1), 0, self.rows))
        self.take(1, self.target(shifted(self.me, 1), 0, self.rows))
        self.take(4, self.target(shifted(self.me, 2), 0, half))
        self.take(5, self.target(shifted(self.me, 2), half, half))

    def finish(self):
        for copy in self.sent:
            copy.wait_send()


def swapped(u):
    lane = lax.broadcasted_iota(jnp.int32, u.shape, 1)
    ahead = pltpu.roll(u, HD - HD // 4, 1)
    behind = pltpu.roll(u, HD // 4, 1)
    return jnp.where(lax.rem(lane, HD // 2) < HD // 4, ahead, behind)


def rotated(u, gain, cosine, sine):
    u = u.astype(jnp.float32)
    u = u * lax.rsqrt(jnp.mean(u * u, axis=-1, keepdims=True) + norm_eps) * gain
    return (u * cosine + swapped(u) * sine).astype(jnp.bfloat16)


def barrier_with(peers):
    barrier = pltpu.get_barrier_semaphore()
    for peer in peers:
        pl.semaphore_signal(barrier, inc=1, device_id=peer, device_id_type=MESH)
    return lambda: pl.semaphore_wait(barrier, len(peers))


def tables():
    lane = np.arange(HD)
    quarter = HD // 4
    inverse_freq = np.float32(rope_base) ** (-(lane % quarter).astype(np.float32) / np.float32(quarter))
    sign = np.where(lane % (HD // 2) < quarter, -1.0, 1.0).astype(np.float32)
    rows = np.arange(16 * TOK // GRID_W, dtype=np.float32)[:, None] * inverse_freq
    columns = np.arange(GRID_W, dtype=np.float32)[:, None] * inverse_freq
    of_row = lane < HD // 2

    def table(angles, used):
        pair = np.stack([np.cos(angles), np.sin(angles) * sign])
        return jnp.asarray(np.where(used, pair, 0.0).astype(np.float32))

    return table(rows, of_row), table(columns, ~of_row)


class RingGather:
    SENDS = 4

    def __init__(self, axis, piece, own, send_sems, recv_sems, base):
        self.axis, self.me = axis, lax.axis_index(axis)
        self.piece, self.own = piece, own
        self.send_sems, self.recv_sems, self.base = send_sems, recv_sems, base
        self.sent = []

    def put(self, k, src, dst, by):
        device = {self.axis: shifted(self.me, by)}
        k += self.base
        self.sent.append(send(src, dst, self.send_sems.at[k], self.recv_sems.at[k], device))

    def take(self, k, dst):
        k += self.base
        arrived(dst, self.send_sems.at[k], self.recv_sems.at[k], {self.axis: self.me})

    def begin(self):
        self.put(0, self.own, self.piece(self.me, None), 1)
        self.put(1, self.own, self.piece(self.me, None), -1)

    def low(self):
        who = shifted(self.me, -1)
        self.take(0, self.piece(who, None))
        self.put(2, self.piece(who, 0), self.piece(who, 0), 1)

    def high(self):
        who = shifted(self.me, 1)
        self.take(1, self.piece(who, None))
        self.put(3, self.piece(who, 1), self.piece(who, 1), -1)

    def far(self):
        who = shifted(self.me, 2)
        self.take(2, self.piece(who, 0))
        self.take(3, self.piece(who, 1))

    def finish(self):
        for copy in self.sent:
            copy.wait_send()


class TorusReduce:
    SENDS = 20

    def __init__(self, first, second, piece, start, rows, bufs, send_sems, recv_sems, base):
        self.first, self.second = first, second
        self.a, self.b = lax.axis_index(first), lax.axis_index(second)
        self.piece, self.start, self.rows = piece, start, rows
        self.buf = bufs
        self.send_sems, self.recv_sems, self.base = send_sems, recv_sems, base
        self.sent = []

    def dest(self, j):
        return shifted(self.b, (2, 1, -1, 0)[j])

    def ref(self, a, b, part):
        rows = self.rows // 2
        if part is None:
            return self.piece(a, b, self.start, self.rows)
        return self.piece(a, b, self.start + part * rows, rows)

    def put(self, k, axis, by, src, dst):
        device = {axis: shifted(lax.axis_index(axis), by)}
        k += self.base
        self.sent.append(send(src, dst, self.send_sems.at[k], self.recv_sems.at[k], device))

    def take(self, k, dst):
        k += self.base
        arrived(dst, self.send_sems.at[k], self.recv_sems.at[k], {self.first: self.a})

    @staticmethod
    def add(into, *others):
        total = into[...].astype(jnp.float32)
        for other in others:
            total = total + other[...].astype(jnp.float32)
        into[...] = total.astype(into.dtype)

    def far(self, j):
        a, b = shifted(self.a, 2), self.dest(j)
        self.put(4 * j, self.first, 1, self.ref(a, b, 0), self.buf("far_first", 0, j))
        self.put(4 * j + 1, self.first, -1, self.ref(a, b, 1), self.buf("far_first", 1, j))

    def up(self, j):
        a, b = shifted(self.a, 1), self.dest(j)
        self.take(4 * j, self.buf("far_first", 0, j))
        self.add(self.ref(a, b, 0), self.buf("far_first", 0, j))
        self.put(4 * j + 2, self.first, 1, self.ref(a, b, None), self.buf("near_first", 0, j))

    def down(self, j):
        a, b = shifted(self.a, -1), self.dest(j)
        self.take(4 * j + 1, self.buf("far_first", 1, j))
        self.add(self.ref(a, b, 1), self.buf("far_first", 1, j))
        self.put(4 * j + 3, self.first, -1, self.ref(a, b, None), self.buf("near_first", 1, j))

    def own(self, j):
        self.take(4 * j + 2, self.buf("near_first", 0, j))
        self.take(4 * j + 3, self.buf("near_first", 1, j))
        self.add(self.ref(self.a, self.dest(j), None), self.buf("near_first", 0, j), self.buf("near_first", 1, j))

    def second_far(self):
        b = shifted(self.b, 2)
        self.put(16, self.second, 1, self.ref(self.a, b, 0), self.buf("far_second", 0, 0))
        self.put(17, self.second, -1, self.ref(self.a, b, 1), self.buf("far_second", 1, 0))

    def second_up(self):
        b = shifted(self.b, 1)
        self.take(16, self.buf("far_second", 0, 0))
        self.add(self.ref(self.a, b, 0), self.buf("far_second", 0, 0))
        self.put(18, self.second, 1, self.ref(self.a, b, None), self.buf("near_second", 0, 0))

    def second_down(self):
        b = shifted(self.b, -1)
        self.take(17, self.buf("far_second", 1, 0))
        self.add(self.ref(self.a, b, 1), self.buf("far_second", 1, 0))
        self.put(19, self.second, -1, self.ref(self.a, b, None), self.buf("near_second", 1, 0))

    def total(self):
        self.take(18, self.buf("near_second", 0, 0))
        self.take(19, self.buf("near_second", 1, 0))
        total = self.ref(self.a, self.b, None)[...].astype(jnp.float32)
        total = total + self.buf("near_second", 0, 0)[...].astype(jnp.float32)
        return total + self.buf("near_second", 1, 0)[...].astype(jnp.float32)

    def finish(self):
        for copy in self.sent:
            copy.wait_send()


def layer_kernel(
    queries, keys, values, documents, query_gain, key_gain, row_table, column_table,
    out_w, residuals, norm_gains, up_w, down_w, mixed,
    x_all, up_all, down_all, sums, theirs, stream, hidden, squared, squares,
    hidden_early, totals, inverse, of_rows, of_columns, docs, doc_column, q_gain, k_gain, gains, send_sems, recv_sems, local_sems, free_sem,
):
    z, x, y, c = (lax.axis_index(n) for n in ("z", "x", "y", "c"))
    other = 1 - c
    sp = z * N + x
    tp = y * 2 + c
    plane = [
        {"z": shifted(z, dz), "x": shifted(x, dx)} for dz in range(N) for dx in range(N) if dz or dx
    ]
    group = [{"y": shifted(y, dy), "c": cc} for dy in range(N) for cc in (c, other) if dy or cc is other]
    wait = barrier_with(plane + group)

    def kv_place(zz, xx, start, rows):
        return sums.at[1, zz, xx, pl.ds(start, rows), :]

    def att_slot(t, part):
        rows = pl.ds(0, TOK) if part is None else pl.ds(part * HALF, HALF)
        return sums.at[0, lax.div(t, 4), lax.rem(t, 4), rows, pl.ds(0, 256)]

    def col_slot(t, start=0, rows=256):
        return theirs.at[lax.div(t, 4), lax.rem(t, 4), pl.ds(start, rows), :]

    def thousand(index):
        return pl.ds(pl.multiple_of(index * TOK, TOK), TOK)

    q_in = theirs.at[2, 0, :, pl.ds(0, 2 * HD)]
    k_in = theirs.at[2, 1, :, pl.ds(0, HD)]
    v_in = theirs.at[2, 2, :, pl.ds(0, HD)]
    q_rot = theirs.at[2, 3]
    residual = theirs.at[3, 0]
    cosine = stream.at[:, pl.ds(2 * HD, HD)]
    sine = stream.at[:, pl.ds(3 * HD, HD)]

    def local(i, src, dst):
        copy = pltpu.make_async_copy(src, dst, local_sems.at[i])
        copy.start()
        return copy

    first = [
        local(0, keys, k_in),
        local(1, values, v_in),
        local(2, row_table.at[:, pl.ds(pl.multiple_of(sp * 8, 8), 8), :], of_rows),
        local(3, column_table, of_columns),
        local(4, key_gain, k_gain),
        local(5, documents, docs.at[sp]),
    ]
    second = [local(6, queries, q_in), local(7, query_gain, q_gain)]
    third = [
        local(8, residuals, residual),
        local(9, norm_gains, gains),
        local(10, out_w.at[:, thousand(tp)], col_slot(tp)),
    ]
    fourth = [
        local(11, up_w.at[:, thousand(x)], up_all.at[z, x]),
        local(12, down_w.at[thousand(x), :], down_all.at[z, x]),
    ]
    for copy in first:
        copy.wait()
    for i in range(TOK // GRID_W):
        grid_row = slice(i * GRID_W, (i + 1) * GRID_W)
        cosine[grid_row, :] = of_rows[0, i : i + 1, :] + of_columns[0]
        sine[grid_row, :] = of_rows[1, i : i + 1, :] + of_columns[1]
    mine = kv_place(z, x, 0, 2 * HD)
    turned = jnp.transpose(rotated(k_in[...], k_gain[...], cosine[...], sine[...]).astype(jnp.float32))
    mine[HD:, :] = turned.astype(jnp.bfloat16)
    for i in range(TOK // HD):
        mine[:HD, i * HD : (i + 1) * HD] = v_in[i * HD : (i + 1) * HD, :]

    def mark(zz, xx):
        row = lax.broadcasted_iota(jnp.int32, (HD, TOK), 0)
        hot = jnp.where(row == docs[zz * N + xx], key_mark, 0.0)
        sums[1, zz, xx, 2 * HD : 3 * HD, :] = hot.astype(jnp.bfloat16)

    mark(z, x)
    column = jnp.broadcast_to(docs[sp].astype(jnp.float32), (HD, TOK))
    doc_column[...] = jnp.transpose(column).astype(jnp.int32)
    wait()

    kvs = TorusGather("x", "z", lambda a, b, s, r: kv_place(b, a, s, r), 0, 2 * HD, send_sems, recv_sems, 0)
    ups_across = Exchange(
        "x",
        lambda to, s, r: up_w.at[pl.ds(s, r), thousand(to)],
        lambda who, s, r: up_all.at[z, who, pl.ds(s, r), :],
        lambda i: squared.at[0, pl.ds(128 * i, 128), :],
        256, send_sems, recv_sems, 20,
    )
    downs_across = Exchange(
        "x",
        lambda to, s, r: down_w.at[pl.ds(pl.multiple_of(to * TOK + s, HALF), r), :],
        lambda who, s, r: down_all.at[z, who, pl.ds(s, r), :],
        lambda i: squared.at[1, pl.ds(256 * i, 256), pl.ds(0, 256)],
        512, send_sems, recv_sems, 26,
    )
    columns = []
    for i, cc in enumerate((c, other)):
        ex = Exchange(
            "y",
            lambda to, s, r, cc=cc: out_w.at[pl.ds(s, r), thousand(to * 2 + cc)],
            lambda who, s, r: col_slot(who * 2 + c, s, r),
            lambda k, i=i: squared.at[2, pl.ds(128 * (2 * i + k), 128), :],
            256, send_sems, recv_sems, 32 + 6 * i, {"c": cc},
        )
        ex.landed = lambda who, s, r, cc=cc: col_slot(who * 2 + cc, s, r)
        columns.append(ex)
    kvs.begin()
    kvs.spread(0)
    doc_copies = [
        send(docs.at[sp], docs.at[sp], send_sems.at[45 + i], recv_sems.at[45 + i], peer)
        for i, peer in enumerate(plane)
    ]
    for ex in columns:
        ex.begin()
    twin = send(
        out_w.at[:, thousand(y * 2 + other)], col_slot(tp), send_sems.at[44], recv_sems.at[44], {"c": other}
    )

    for copy in second:
        copy.wait()
    lane = lax.broadcasted_iota(jnp.int32, (TOK, HD), 1)
    hot = jnp.where(lane == doc_column[...], query_mark, 0.0).astype(jnp.bfloat16)
    for h in range(2):
        turn = rotated(q_in[:, h * HD : (h + 1) * HD], q_gain[...], cosine[...], sine[...])
        for t in range(2):
            rows, part = slice(h * HALF, (h + 1) * HALF), slice(t * HALF, (t + 1) * HALF)
            q_rot[rows, 2 * t * HD : (2 * t + 1) * HD] = turn[part]
            q_rot[rows, (2 * t + 1) * HD : (2 * t + 2) * HD] = hot[part]
    hidden[:, :HD] = jnp.zeros((2 * TOK, HD), jnp.float32)
    hidden[:, HD : 2 * HD] = jnp.full((2 * TOK, HD), masked_score, jnp.float32)
    hidden[:, 2 * HD : 3 * HD] = jnp.zeros((2 * TOK, HD), jnp.float32)
    scale = HD ** (-0.5) * 1.4426950408889634

    def attend(count, which):
        @pl.loop(0, 2)
        def _(t):
            rows = pl.ds(pl.multiple_of(t * TOK, TOK), TOK)
            q = q_rot[:, pl.ds(pl.multiple_of(t * HALF, HALF), HALF)]
            cuts = [slice(i * HD, (i + 1) * HD) for i in range(4)]

            def step(i, carry):
                top, total, weighted = carry
                zz, xx = which(i)
                packed = sums[1, zz, xx, :HD, :]
                v = jnp.concatenate([packed[:, cut] for cut in cuts], axis=0)
                s = jnp.dot(q, sums[1, zz, xx, HD : 3 * HD, :], preferred_element_type=jnp.float32)
                s = [s[:, cut] for cut in cuts]
                most = jnp.maximum(jnp.maximum(s[0], s[1]), jnp.maximum(s[2], s[3]))
                new_top = jnp.maximum(top, jnp.max(most, axis=-1, keepdims=True))
                p = [jnp.exp2((part - new_top) * scale) for part in s]
                fade = jnp.exp2((top - new_top) * scale)
                total = total * fade + ((p[0] + p[1]) + (p[2] + p[3]))
                low = jnp.concatenate([part.astype(jnp.bfloat16) for part in p], axis=1)
                weighted = weighted * fade + jnp.dot(low, v, preferred_element_type=jnp.float32)
                return new_top, total, weighted

            start = (hidden[rows, cuts[1]], hidden[rows, cuts[2]], hidden[rows, cuts[0]])
            top, total, weighted = lax.fori_loop(0, count, step, start)
            hidden[rows, cuts[1]] = top
            hidden[rows, cuts[2]] = total
            hidden[rows, cuts[0]] = weighted

    attend(1, lambda i: (z, x))
    kvs.near()
    kvs.far()
    ups_across.begin()
    downs_across.begin()
    for i, peer in enumerate(plane):
        dz, dx = divmod(i + 1, N)
        arrived(
            docs.at[shifted(z, -dz) * N + shifted(x, -dx)], send_sems.at[45 + i], recv_sems.at[45 + i], {"z": z}
        )

    @pl.loop(1, 16)
    def _(i):
        mark(lax.rem(z + lax.div(i, N), N), lax.rem(x + i, N))

    attend(3, lambda i: (z, lax.rem(x + 1 + i, N)))
    kvs.pass_on(0)
    kvs.pass_on(1)
    for ex in columns:
        ex.pass_on()
    attend(4, lambda i: (lax.rem(z + 1 + 2 * lax.rem(i, 2), N), lax.rem(x + N - lax.div(i, 2), N)))
    kvs.pass_on(2)
    kvs.pass_on(3)
    ups_across.pass_on()
    downs_across.pass_on()
    attend(4, lambda i: (lax.rem(z + 1 + 2 * lax.rem(i, 2), N), lax.rem(x + 1 + lax.div(i, 2), N)))
    kvs.last(0)
    kvs.last(1)
    attend(2, lambda i: (lax.rem(z + 2, N), lax.rem(x + N - i, N)))
    kvs.last(2)
    kvs.last(3)
    def half_of(ref, z_at, part):
        at = ref.at[z_at]
        return at if part is None else at.at[pl.ds(2 * part, 2)]

    ups = RingGather(
        "z", lambda who, part: half_of(up_all, who, part), up_all.at[z], send_sems, recv_sems, 68
    )
    downs = RingGather(
        "z", lambda who, part: half_of(down_all, who, part), down_all.at[z], send_sems, recv_sems, 72
    )
    for copy in fourth:
        copy.wait()
    ups_across.last()
    ups.begin()
    attend(2, lambda i: (lax.rem(z + 2, N), lax.rem(x + 1 + i, N)))

    att = att_slot(tp, None)
    for t in range(2):
        for h in range(2):
            rows = slice(t * TOK + h * HALF, t * TOK + (h + 1) * HALF)
            total = jnp.sum(hidden[rows, 2 * HD : 3 * HD], axis=-1, keepdims=True)
            att[t * HALF : (t + 1) * HALF, h * HD : (h + 1) * HD] = (hidden[rows, :HD] / total).astype(jnp.bfloat16)

    handed = []

    def hand(k, src, dst):
        handed.append(send(src, dst, send_sems.at[k], recv_sems.at[k], {"c": other}))

    def taken(k, dst):
        arrived(dst, send_sems.at[k], recv_sems.at[k], {"c": c})

    heads_sent = []

    def pass_heads(k, who, part, by):
        ref = att_slot(who * 2 + c, part)
        heads_sent.append(send(ref, ref, send_sems.at[k], recv_sems.at[k], {"y": shifted(y, by)}))

    def take_heads(k, who, part):
        taken(k, att_slot(who * 2 + c, part))

    pass_heads(60, y, 0, 1)
    pass_heads(61, y, 1, -1)
    hand(64, att, att)

    for copy in third:
        copy.wait()
    for ex in columns:
        ex.target = ex.landed
        ex.last()
    arrived(col_slot(y * 2 + other), send_sems.at[44], recv_sems.at[44], {"c": c})

    def project(t):
        part = jnp.dot(att_slot(t, None)[...], col_slot(t)[...], preferred_element_type=jnp.float32)
        stream[...] += part.astype(jnp.bfloat16).astype(jnp.float32)

    y_low, y_high, y_far = shifted(y, -1), shifted(y, 1), shifted(y, 2)
    stream[...] = residual[...].astype(jnp.float32)
    for copy in heads_sent:
        copy.wait_send()
    heads_sent.clear()
    pass_heads(214, y, 1, 1)
    pass_heads(215, y, 0, -1)
    project(tp)
    take_heads(60, y_low, 0)
    pass_heads(62, y_low, 0, 1)
    take_heads(61, y_high, 1)
    pass_heads(63, y_high, 1, -1)
    take_heads(214, y_low, 1)
    hand(65, att_slot(y_low * 2 + c, None), att_slot(y_low * 2 + c, None))
    take_heads(215, y_high, 0)
    hand(66, att_slot(y_high * 2 + c, None), att_slot(y_high * 2 + c, None))
    taken(64, att_slot(y * 2 + other, None))
    project(y * 2 + other)
    project(y_low * 2 + c)
    project(y_high * 2 + c)
    downs_across.last()
    take_heads(62, y_far, 0)
    take_heads(63, y_far, 1)
    hand(67, att_slot(y_far * 2 + c, None), att_slot(y_far * 2 + c, None))
    taken(65, att_slot(y_low * 2 + other, None))
    project(y_low * 2 + other)
    taken(66, att_slot(y_high * 2 + other, None))
    project(y_high * 2 + other)
    project(y_far * 2 + c)
    taken(67, att_slot(y_far * 2 + other, None))
    project(y_far * 2 + other)

    x_all[x, tp] = (stream[...] * gains[tp]).astype(jnp.bfloat16)

    def place(xx, yy, start, rows):
        return x_all.at[xx, yy * 2 + c, pl.ds(start, rows), :]

    gathers = [
        TorusGather("y", "x", lambda a, b, s, r: place(b, a, s, r), 0, HALF, send_sems, recv_sems, 83),
        TorusGather("x", "y", place, HALF, HALF, send_sems, recv_sems, 103),
    ]

    def share(n, j, i):
        g = gathers[n]
        ref = g.ref(g.order(j), shifted(g.b, (0, -1, 1, 2)[i]), None)
        hand(123 + 16 * n + 4 * j + i, ref, ref)

    def shared(n, j, i):
        g = gathers[n]
        a, b = g.order(j), shifted(g.b, (0, -1, 1, 2)[i])
        xx, yy = (b, a) if n == 0 else (a, b)
        taken(123 + 16 * n + 4 * j + i, x_all.at[xx, yy * 2 + other, pl.ds(n * HALF, HALF), :])

    def weight(t):
        return up_all[lax.div(t, 2), pl.ds(2 * lax.rem(t, 2), 2)].reshape(TOK, TOK)

    def square(value, scales):
        positive = jnp.maximum(value, 0.0) * jnp.concatenate([scales] * (TOK // HD), axis=1)
        return (positive * positive).astype(jnp.bfloat16)

    def early(blocks, first, count, step, clear, store):
        rows = HALF * len(blocks)
        acc = hidden_early.at[pl.ds(0, rows)]
        if clear:
            acc[...] = jnp.zeros_like(acc)

        @pl.loop(0, count)
        def _(i):
            t = lax.rem(first + step * i, 8)
            parts = [x_all[xx, t, :HALF, :] for xx in blocks]
            part = parts[0] if len(parts) == 1 else jnp.concatenate(parts, axis=0)
            acc[...] += jnp.dot(part, weight(t), preferred_element_type=jnp.float32)

        if store:
            for i, xx in enumerate(blocks):
                squared[xx, :HALF, :] = square(
                    hidden_early[i * HALF : (i + 1) * HALF, :], inverse[xx, :HALF, :]
                )

    def late(first, count, step):
        @pl.loop(0, count)
        def _(i):
            t = lax.rem(first + step * i, 8)
            rows = x_all[:, t, HALF:, :].reshape(N * HALF, TOK)
            hidden[...] += jnp.dot(rows, weight(t), preferred_element_type=jnp.float32)

    for g in gathers:
        g.begin()
    for n in range(2):
        share(n, 0, 0)
    whole = stream[...]
    partial = jnp.sum(whole * whole, axis=-1, keepdims=True)
    squares[tp] = jnp.transpose(jnp.broadcast_to(partial, (TOK, HD)))[:8]
    square_copies = [
        send(squares.at[tp], squares.at[tp], send_sems.at[76 + i], recv_sems.at[76 + i], peer)
        for i, peer in enumerate(group)
    ]
    ups.low()
    ups.high()
    downs.begin()
    for g in gathers:
        g.follow()
    for done in (kvs, ups_across, downs_across, *columns):
        done.finish()
    for copy in (*handed[:4], *heads_sent, *doc_copies, twin):
        copy.wait_send()
    del handed[:4]
    i = 0
    for dy in range(N):
        for cc in (c, other):
            if dy or cc is other:
                arrived(squares.at[shifted(y, -dy) * 2 + cc], send_sems.at[76 + i], recv_sems.at[76 + i], {"c": c})
                i += 1
    full = squares[0]
    for t in range(1, 8):
        full = full + squares[t]
    totals[x] = full
    hidden[...] = jnp.zeros_like(hidden)
    for n, g in enumerate(gathers):
        g.near()
        share(n, 1, 0)
        share(n, 2, 0)
    square_copies += [
        send(totals.at[x], totals.at[x], send_sems.at[210 + dx], recv_sems.at[210 + dx], {"x": shifted(x, dx)})
        for dx in range(1, N)
    ]
    for n, g in enumerate(gathers):
        g.far()
        share(n, 3, 0)
    for dx in range(1, N):
        arrived(totals.at[shifted(x, -dx)], send_sems.at[210 + dx], recv_sems.at[210 + dx], {"x": x})
    for xx in range(N):
        full = jnp.transpose(jnp.broadcast_to(totals[xx, :1, :], (HD, TOK)))
        inverse[xx] = lax.rsqrt(full / D + norm_eps)
    ups.far()
    for n in range(2):
        for j in range(N):
            shared(n, j, 0)
        if n == 0:
            early([x], 0, 8, 1, True, True)
    for j in range(N):
        for n, g in enumerate(gathers):
            g.pass_on(j)
            share(n, j, 1)
            share(n, j, 2)
    late(2 * (y + 3) + c, 3, 2)
    late(2 * y + other, 1, 2)
    for j in range(N):
        for i in (1, 2):
            for n in range(2):
                shared(n, j, i)
    late(2 * (y + 3) + other, 2, 4)
    downs.low()
    downs.high()
    sides = [shifted(x, -1), shifted(x, 1)]
    early(sides, 0, 4, 1, True, False)
    for j in range(N):
        for n, g in enumerate(gathers):
            g.last(j)
            share(n, j, 3)
    early(sides, 4, 4, 1, False, True)
    opposite = [shifted(x, 2)]
    late(2 * (y + 2) + c, 1, 2)
    early(opposite, c, 4, 2, True, False)
    for n in range(2):
        for j in range(N):
            shared(n, j, 3)
    early(opposite, other, 4, 2, False, True)
    late(2 * (y + 2) + other, 1, 2)
    @pl.loop(0, N)
    def _(xx):
        rows = pl.ds(pl.multiple_of(xx * HALF, HALF), HALF)
        squared[xx, HALF:, :] = square(hidden[rows, :], inverse[xx, HALF:, :])

    for g in gathers:
        g.finish()
    for copy in handed:
        copy.wait_send()
    handed.clear()
    for peer in ({"x": shifted(x, 1)}, {"x": shifted(x, -1)}, {"y": shifted(y, 1)}, {"y": shifted(y, -1)}):
        pl.semaphore_signal(free_sem, inc=1, device_id=peer, device_id_type=MESH)

    def column(cc, xx, yy):
        pair = [down_all[yy, 2 * cc + part] for part in range(2)]
        sums[cc, xx, yy] = jnp.dot(
            squared[xx], jnp.concatenate(pair, axis=1), preferred_element_type=jnp.float32
        ).astype(jnp.bfloat16)

    def near_columns(cc, xx):
        @pl.loop(0, N - 1)
        def _(i):
            column(cc, xx, lax.rem(z + 3 + i, N))

    def far_column(cc, xx):
        column(cc, xx, shifted(z, 2))

    def hand_on(i, xx, offsets):
        for k in offsets:
            yy = shifted(z, k)
            hand((155, 199, 203, 207)[i] + k % N, sums.at[other, xx, yy], theirs.at[xx, yy])

    def joined(i, xx):
        for k in range(N):
            taken((155, 199, 203, 207)[i] + k, theirs.at[xx, shifted(z, k)])

        @pl.loop(0, N)
        def _(yy):
            TorusReduce.add(sums.at[c, xx, yy], theirs.at[xx, yy])

    def sum_place(xx, yy, start, rows):
        return sums.at[c, xx, yy, pl.ds(start, rows), :]

    def bufs(n):
        def buf(kind, way, j):
            if kind == "near_first":
                return x_all.at[n, 4 * way + j, pl.ds(0, HALF), :]
            if kind == "far_first":
                return x_all.at[n, 4 * way + j, pl.ds(HALF, HALF // 2), :]
            if kind == "near_second":
                return x_all.at[2, 2 * n + way, pl.ds(0, HALF), :]
            return x_all.at[2, 2 * n + way, pl.ds(HALF, HALF // 2), :]

        return buf

    rows_x = TorusReduce("x", "y", sum_place, 0, HALF, bufs(0), send_sems, recv_sems, 159)
    rows_y = TorusReduce(
        "y", "x", lambda a, b, s, r: sum_place(b, a, s, r), HALF, HALF, bufs(1), send_sems, recv_sems, 179
    )
    blocks = [rows_y.dest(j) for j in range(N)]
    for i in range(2):
        near_columns(other, blocks[i])
        hand_on(i, blocks[i], (-1, 0, 1))
    near_columns(c, blocks[0])
    downs.far()
    far_column(other, blocks[0])
    hand_on(0, blocks[0], (2,))
    far_column(c, blocks[0])
    far_column(other, blocks[1])
    hand_on(1, blocks[1], (2,))
    pl.semaphore_wait(free_sem, 4)
    joined(0, blocks[0])
    for j in range(N):
        rows_x.far(j)
    rows_y.far(0)
    near_columns(c, blocks[1])
    far_column(c, blocks[1])
    joined(1, blocks[1])
    rows_y.far(1)
    near_columns(other, blocks[2])
    far_column(other, blocks[2])
    hand_on(2, blocks[2], (-1, 0, 1, 2))
    rows_y.up(0)
    rows_y.down(0)
    near_columns(c, blocks[2])
    far_column(c, blocks[2])
    near_columns(other, blocks[3])
    far_column(other, blocks[3])
    hand_on(3, blocks[3], (-1, 0, 1, 2))
    joined(2, blocks[2])
    rows_y.far(2)
    rows_y.up(1)
    rows_y.down(1)
    near_columns(c, blocks[3])
    far_column(c, blocks[3])
    joined(3, blocks[3])
    rows_y.far(3)
    for j in range(2):
        rows_x.up(j)
        rows_x.down(j)
    rows_y.up(2)
    rows_y.down(2)
    rows_y.own(0)
    rows_y.second_far()
    for j in range(2, N):
        rows_x.up(j)
        rows_x.down(j)
    rows_y.up(3)
    rows_y.down(3)
    rows_y.own(1)
    rows_y.second_up()
    rows_x.own(0)
    rows_x.second_far()
    rows_x.own(1)
    rows_y.own(2)
    rows_y.second_down()
    rows_x.second_up()
    rows_x.own(2)
    rows_x.second_down()
    rows_y.own(3)
    rows_x.own(3)
    mixed[:HALF, :] = (stream[:HALF, :] + rows_x.total()).astype(jnp.bfloat16)
    mixed[HALF:, :] = (stream[HALF:, :] + rows_y.total()).astype(jnp.bfloat16)
    for done in (ups, downs, rows_x, rows_y):
        done.finish()
    for copy in (*handed, *square_copies):
        copy.wait_send()


def body(
    queries, keys, values, documents, query_gain, key_gain, residual, out_weight, norm_gain, up_weight, down_weight
):
    bf, f32 = jnp.bfloat16, jnp.float32
    row_table, column_table = tables()
    return pl.pallas_call(
        layer_kernel,
        out_shape=jax.ShapeDtypeStruct((TOK, TOK), bf),
        in_specs=[ANY] * 13,
        out_specs=VMEM,
        scratch_shapes=[
            pltpu.VMEM((N, 8, TOK, TOK), bf),
            pltpu.VMEM((N, N, 256, TOK), bf),
            pltpu.VMEM((N, N, TOK, 256), bf),
            pltpu.VMEM((2, N, N, TOK, TOK), bf),
            pltpu.VMEM((N, N, TOK, TOK), bf),
            pltpu.VMEM((TOK, TOK), f32),
            pltpu.VMEM((N * HALF, TOK), f32),
            pltpu.VMEM((N, TOK, TOK), bf),
            pltpu.VMEM((8, 8, TOK), f32),
            pltpu.VMEM((TOK, TOK), f32),
            pltpu.VMEM((N, 8, TOK), f32),
            pltpu.VMEM((N, TOK, HD), f32),
            pltpu.VMEM((2, TOK // GRID_W, HD), f32),
            pltpu.VMEM((2, GRID_W, HD), f32),
            pltpu.VMEM((16, 1, TOK), jnp.int32),
            pltpu.VMEM((TOK, HD), jnp.int32),
            pltpu.VMEM((1, HD), f32),
            pltpu.VMEM((1, HD), f32),
            pltpu.VMEM((8, 1, TOK), f32),
            pltpu.SemaphoreType.DMA((216,)),
            pltpu.SemaphoreType.DMA((216,)),
            pltpu.SemaphoreType.DMA((13,)),
            pltpu.SemaphoreType.REGULAR,
        ],
        compiler_params=pltpu.CompilerParams(
            collective_id=0, has_side_effects=True, vmem_limit_bytes=67043328
        ),
        name="layer",
    )(
        queries, keys, values, documents.reshape(1, TOK), query_gain.reshape(1, HD), key_gain.reshape(1, HD),
        row_table, column_table, out_weight, residual, norm_gain.reshape(8, 1, TOK), up_weight, down_weight,
    )


def solution(mesh):
    split = Mesh(mesh.devices.reshape(N, N, N, 2), ("z", "x", "y", "c"))
    sp, tp = ("z", "x"), ("y", "c")
    return jax.shard_map(
        body,
        mesh=split,
        in_specs=(
            P(sp, tp), P(sp, tp), P(sp, tp), P(sp), P(), P(), P(sp, tp), P(tp, None), P(), P(sp, tp), P(tp, sp),
        ),
        out_specs=P(sp, tp),
        check_vma=False,
    )
```
